128 devices in a mesh: rep: 2 (over z_hi), fs: 32 (over z_lo, y, x), tp: 2 (over core).
Axes of the slice: x: 4, y: 4, z: 4 (z_hi: 2, z_lo: 2; z = z_hi * 2 + z_lo), core: 2. Of those that a mesh axis runs over, the one named last changes fastest.
Arguments:
- later_input: bfloat16 [32768, 2048], P(('rep', 'fs', 'tp')), may hold values from -6 to 6
- earlier_input: bfloat16 [32768, 2048], P(('rep', 'fs', 'tp')), may hold values from -6 to 6
- hidden_cot: bfloat16 [32768, 2816], P(('rep', 'fs'), 'tp'), may hold values from -8 to 8
- norm_gain: float32 [2048], replicated, may hold values from 0.1 to 1.9
- gate_weight: bfloat16 [2048, 2816], P('fs', 'tp'), may hold values from -0.125 to 0.125
- up_weight: bfloat16 [2048, 2816], P('fs', 'tp'), may hold values from -0.125 to 0.125
- gate_running: float32 [2048, 2816], P('fs', 'tp'), may hold values from -6 to 6
- up_running: float32 [2048, 2816], P('fs', 'tp'), may hold values from -6 to 6
- gain_running: float32 [2048], replicated, may hold values from -6 to 6
Outputs:
- later_hidden: bfloat16 [32768, 2816], P(('rep', 'fs'), 'tp')
- earlier_grad: bfloat16 [32768, 2048], P(('rep', 'fs', 'tp'))
- gate_total: float32 [2048, 2816], P('fs', 'tp')
- up_total: float32 [2048, 2816], P('fs', 'tp')
- gain_total: float32 [2048], replicated
The draws below stay inside these ranges and needn't reach their ends.
All inputs are finite; a program needn't handle non-finite values.
Results may differ from the reference program's by a relative error of at most 0.015.
Values may be sent and summed in bfloat16 or wider, within the bound.
A program may use at most 128 MiB of HBM per device.

```python
import math
import jax
import jax.numpy as jnp
from jax import lax

D = 2048
HIDDEN_SIZE = 2816
HIDDEN_TP = 1408
TOKENS = 32768
N_TP = 2


def raised(array, stream_key, source, target, shards_of, factor):
    owner, partner = [(jnp.arange(array.shape[dim]) // (array.shape[dim] // shards_of)).reshape([-1 if axis == dim else 1 for axis in range(array.ndim)]) for dim in (source, target)]
    chosen = jax.random.permutation(stream_key, shards_of)[partner]
    strong = (owner == chosen) | (owner == (partner + shards_of // 2) % shards_of)
    return jnp.where(strong, factor * array, array)


def shard_levels(rng, shape, cuts, smallest, largest):
    def one(axis_at, blocks):
        steps = jax.random.uniform(jax.random.fold_in(jax.random.fold_in(rng, 6), axis_at), (blocks,), jnp.float32, smallest / len(cuts), largest / len(cuts))
        return jnp.repeat(jnp.exp(steps), shape[axis_at] // blocks).reshape((-1,) + (1,) * (len(shape) - axis_at - 1))

    gain = one(*cuts[0])
    for cut in cuts[1:]:
        gain = gain * one(*cut)
    return gain


def normal_values(key, dims, spread, reach, split=(), kind=jnp.bfloat16):
    array = jax.random.normal(key, dims, jnp.float32) * spread
    if len(split) > 0:
        array = shard_levels(key, dims, split, -0.22, 0.18) * array
    return jnp.clip(array, min=-reach, max=reach).astype(kind)


def bell_draw_with(rng, dims, scale, bound, shards, heavy, dtype=jnp.bfloat16):
    values = scale * jax.random.normal(rng, dims, jnp.float32)
    if shards:
        values = values * shard_levels(rng, dims, shards, -0.22, 0.18)
    return jnp.clip(raised(values, jax.random.fold_in(rng, 3), *heavy), -bound, bound).astype(dtype)


def setup_inputs(seed: int = 0) -> dict:
    seeds = jax.random.split(jax.random.key(seed), 10)
    return {
        "later_input": normal_values(seeds[0], (TOKENS, D), 1.0, 6.0, ((0, 128),)),
        "earlier_input": normal_values(seeds[1], (TOKENS, D), 1.0, 6.0, ((0, 128),)),
        "hidden_cot": bell_draw_with(seeds[2], (TOKENS, HIDDEN_SIZE), 1.0, 8.0, ((0, 64), (1, 2)), (0, 1, 64, 4.0)),
        "norm_gain": jnp.clip(1.0 + 0.18 * jax.random.normal(seeds[3], (D,), jnp.float32), 0.1, 1.9),
        "gate_weight": normal_values(seeds[4], (D, HIDDEN_SIZE), D ** -0.5, 0.125, ((0, 32), (1, 2))),
        "up_weight": normal_values(seeds[5], (D, HIDDEN_SIZE), D ** -0.5, 0.125, ((0, 32), (1, 2))),
        "gate_running": normal_values(seeds[6], (D, HIDDEN_SIZE), 1.0, 6.0, ((0, 32), (1, 2)), jnp.float32),
        "up_running": normal_values(seeds[7], (D, HIDDEN_SIZE), 1.0, 6.0, ((0, 32), (1, 2)), jnp.float32),
        "gain_running": normal_values(seeds[8], (D,), 1.0, 6.0, (), jnp.float32),
    }


EPSILON = 1e-06

def normalize(activation, norm_gain):
    values = activation.astype(jnp.float32)
    inv_rms = lax.rsqrt(lax.optimization_barrier(jnp.mean(values * values, axis=1, keepdims=True)) + EPSILON)
    return (values, inv_rms, (values * inv_rms * norm_gain).astype(jnp.bfloat16))

def reference(later_input, earlier_input, hidden_cot, norm_gain, gate_weight, up_weight, gate_running, up_running, gain_running):
    factor = 1.0 / math.sqrt(TOKENS)
    later_vals, later_inv, later_norm = normalize(later_input, norm_gain)
    later_gate = jnp.dot(later_norm, gate_weight, preferred_element_type=jnp.float32)
    later_up = jnp.dot(later_norm, up_weight, preferred_element_type=jnp.float32)
    later_hidden = (jax.nn.silu(later_gate) * later_up).astype(jnp.bfloat16)
    earlier_vals, earlier_inv, earlier_norm = normalize(earlier_input, norm_gain)
    earlier_gate = jnp.dot(earlier_norm, gate_weight, preferred_element_type=jnp.float32)
    earlier_up = jnp.dot(earlier_norm, up_weight, preferred_element_type=jnp.float32)
    gate_sigmoid = jax.nn.sigmoid(earlier_gate)
    upstream = hidden_cot.astype(jnp.float32)
    d_up = (upstream * earlier_gate * gate_sigmoid).astype(jnp.bfloat16)
    d_gate = (upstream * earlier_up * gate_sigmoid * (1.0 + earlier_gate * (1.0 - gate_sigmoid))).astype(jnp.bfloat16)
    d_norm = jnp.zeros((TOKENS, D), jnp.float32)
    for column_block in range(N_TP):
        first_col = column_block * HIDDEN_TP
        partial_sum = jnp.dot(d_gate[:, first_col:first_col + HIDDEN_TP], gate_weight[:, first_col:first_col + HIDDEN_TP].T, preferred_element_type=jnp.float32)
        partial_sum = partial_sum + jnp.dot(d_up[:, first_col:first_col + HIDDEN_TP], up_weight[:, first_col:first_col + HIDDEN_TP].T, preferred_element_type=jnp.float32)
        rounded = lax.optimization_barrier(partial_sum.astype(jnp.bfloat16))
        d_norm = d_norm + rounded.astype(jnp.float32)
    scaled = d_norm * norm_gain
    inner = lax.optimization_barrier(jnp.mean(scaled * earlier_vals, axis=1, keepdims=True))
    earlier_grad = (earlier_inv * scaled - earlier_vals * earlier_inv ** 3 * inner).astype(jnp.bfloat16)
    gate_total = gate_running + factor * jnp.dot(earlier_norm.T, d_gate, preferred_element_type=jnp.float32)
    up_total = up_running + factor * jnp.dot(earlier_norm.T, d_up, preferred_element_type=jnp.float32)
    gain_total = gain_running + factor * lax.optimization_barrier(jnp.sum(d_norm * earlier_vals * earlier_inv, axis=0))
    return (later_hidden, earlier_grad, gate_total, up_total, gain_total)
```

```python
import functools
import math

import jax
import jax.numpy as jnp
from jax import lax
from jax.experimental import pallas as pl
from jax.experimental.pallas import tpu as pltpu
from jax.sharding import PartitionSpec as P

EPSILON = 1e-06
MESH = pl.DeviceIdType.MESH
HALF = 128
F32, BF16 = jnp.float32, jnp.bfloat16
SIZE = {"z": 2, "y": 4, "x": 4}
ORDERS = (("y", "z", "x"), ("x", "z", "y"), ("x", "y", "z"), ("y", "x", "z"))
ALL = slice(None)


def sigmoid(v):
    return 1.0 / (1.0 + jnp.exp(-v))


def landing_shapes(blocks, quarter):
    shapes = []
    for order in ORDERS:
        full = [a for a in "zyx"]
        for axis in reversed(order):
            full.remove(axis)
            lead = tuple(SIZE[a] for a in full)
            if axis == "z":
                shapes.append((blocks, 2, *lead, quarter, HALF))
            else:
                shapes.append((blocks, 2, *lead, quarter, HALF))
                shapes.append((blocks, 2, *lead, quarter, 2 * HALF))
    return shapes


def kernel(
    blocks, factor, later_hbm, earlier_hbm, cot_hbm, gain_ref, gw_hbm, uw_hbm, grun_hbm, urun_hbm, gain_run,
    hidden_hbm, grad_hbm, gtot_hbm, utot_hbm, gain_tot,
    w, g, xin, xl, xe, xt, cot, d, acc, lh, dn, inv_ref, run, gbuf, rep_in, *rest,
):
    landing = list(rest[:-10])
    ag_send, ag_recv, rs_send, rs_recv, load_sem, w_sem, tp_send, tp_recv, gs, out_sem = rest[-10:]
    gain_send, gain_recv = gs.at[0], gs.at[1]
    rows = xin.shape[1]
    width = xin.shape[2]
    quarter = g.shape[4] // 4
    rep, fs, tp = lax.axis_index("rep"), lax.axis_index("fs"), lax.axis_index("tp")
    own = {"x": fs % 4, "y": (fs // 4) % 4, "z": fs // 16}
    ring_z = 2 * rep + own["z"]

    def peer(axis, by):
        if axis == "z":
            z = (ring_z + by) % 4
            return {"rep": z // 2, "fs": (z % 2) * 16 + own["y"] * 4 + own["x"]}
        c = (own[axis] + by) % 4
        if axis == "y":
            return {"fs": own["z"] * 16 + c * 4 + own["x"]}
        return {"fs": own["z"] * 16 + own["y"] * 4 + c}

    def shifted(axis, by):
        return (1 - own["z"] if by else own["z"]) if axis == "z" else (own[axis] + by) % 4

    HALVES = (pl.ds(0, HALF), pl.ds(HALF, HALF), pl.ds(0, 2 * HALF))

    def region(j, q, sel, half):
        return (j, sel["z"], sel["y"], sel["x"], pl.ds(q * quarter, quarter), HALVES[half])

    def sel_of(full, axis, coordinate):
        s = {a: (ALL if a in full else own[a]) for a in "zyx"}
        s[axis] = coordinate
        return s

    ag_plan = []
    count = 0
    for q, order in enumerate(ORDERS):
        phases = []
        for p, axis in enumerate(order):
            full = order[:p]
            if axis == "z":
                group = []
                for k, by in enumerate((1, -1)):
                    group.append((count, (q, sel_of(full, "z", own["z"]), k), ("z", by), (q, sel_of(full, "z", 1 - own["z"]), k)))
                    count += 1
                phases.append(("z", [group]))
            else:
                first, second = [], []
                for k, by in enumerate((1, -1)):
                    first.append((count, (q, sel_of(full, axis, own[axis]), 2), (axis, by), (q, sel_of(full, axis, shifted(axis, -by)), 2)))
                    count += 1
                for k, by in enumerate((1, -1)):
                    second.append((count, (q, sel_of(full, axis, shifted(axis, -by)), k), (axis, by), (q, sel_of(full, axis, shifted(axis, 2)), k)))
                    count += 1
                phases.append((axis, [first, second]))
        ag_plan.append([group for _, groups in phases for group in groups])

    def ag_start(j, t):
        i, src, to, _ = t
        pltpu.make_async_remote_copy(
            src_ref=w.at[region(j, *src)], dst_ref=w.at[region(j, *src)], send_sem=ag_send.at[j, i], recv_sem=ag_recv.at[j, i],
            device_id=peer(*to), device_id_type=MESH,
        ).start()

    def ag_wait(j, t):
        i, src, to, dst = t
        pltpu.make_async_remote_copy(
            src_ref=w.at[region(j, *src)], dst_ref=w.at[region(j, *dst)], send_sem=ag_send.at[j, i], recv_sem=ag_recv.at[j, i],
            device_id=peer(*to), device_id_type=MESH,
        ).wait()

    def ag_stage(j, s):
        for plan in ag_plan:
            if s >= 1:
                for t in plan[s - 1]:
                    ag_wait(j, t)
            if s < len(plan):
                for t in plan[s]:
                    ag_start(j, t)

    rs_plan = []
    count, place = 0, 0
    for q, order in enumerate(ORDERS):
        groups = []
        full = ["z", "y", "x"]
        for axis in reversed(order):
            full.remove(axis)
            if axis == "z":
                group = []
                for k, by in enumerate((1, -1)):
                    group.append((count, (q, sel_of(full, "z", 1 - own["z"]), k), ("z", by), place, k, (q, sel_of(full, "z", own["z"]), k)))
                    count += 1
                groups.append(group)
                place += 1
            else:
                first, second = [], []
                for k, by in enumerate((1, -1)):
                    first.append((count, (q, sel_of(full, axis, shifted(axis, 2)), k), (axis, by), place, k, (q, sel_of(full, axis, shifted(axis, by)), k)))
                    count += 1
                for k, by in enumerate((1, -1)):
                    second.append((count, (q, sel_of(full, axis, shifted(axis, by)), 2), (axis, by), place + 1, k, (q, sel_of(full, axis, own[axis]), 2)))
                    count += 1
                groups += [first, second]
                place += 2
        rs_plan.append(groups)
    rep_index = count

    def rs_copy(j, t):
        i, src, to, at, slot, _ = t
        return pltpu.make_async_remote_copy(
            src_ref=g.at[region(j, *src)], dst_ref=landing[at].at[j, slot], send_sem=rs_send.at[j, i], recv_sem=rs_recv.at[j, i],
            device_id=peer(*to), device_id_type=MESH,
        )

    def rep_copy(j):
        return pltpu.make_async_remote_copy(
            src_ref=g.at[j, own["z"], own["y"], own["x"]], dst_ref=rep_in.at[j], send_sem=rs_send.at[j, rep_index],
            recv_sem=rs_recv.at[j, rep_index], device_id=peer("z", 2), device_id_type=MESH,
        )

    def rs_stage(j, s):
        for plan in rs_plan:
            if s >= 1:
                for t in plan[s - 1]:
                    rs_copy(j, t).wait()
                    _, _, _, at, slot, target = t
                    to = region(j, *target)
                    g[to] = (g[to].astype(F32) + landing[at][j, slot].astype(F32)).astype(BF16)
            if s < len(plan):
                for t in plan[s]:
                    rs_copy(j, t).start()
        if s == 5:
            rep_copy(j).start()

    def rs_finish(j):
        rep_copy(j).wait()
        total = g[j, own["z"], own["y"], own["x"]].astype(F32) + rep_in[j].astype(F32)
        columns = pl.ds(pl.multiple_of(j * HALF, HALF), HALF)
        run[0, :, columns] = run[0, :, columns] + factor * total[:, :HALF]
        run[1, :, columns] = run[1, :, columns] + factor * total[:, HALF:]

    def tp_copy(i, ref):
        return pltpu.make_async_remote_copy(
            src_ref=ref, dst_ref=ref, send_sem=tp_send.at[i], recv_sem=tp_recv.at[i], device_id={"tp": 1 - tp}, device_id_type=MESH
        )

    def tp_received(i, ref):
        return pltpu.make_async_remote_copy(
            src_ref=ref, dst_ref=ref, send_sem=tp_send.at[i], recv_sem=tp_recv.at[i], device_id={"tp": 1 - tp}, device_id_type=MESH
        )

    def dn_copy():
        return pltpu.make_async_remote_copy(
            src_ref=dn.at[1], dst_ref=dn.at[2], send_sem=tp_send.at[3], recv_sem=tp_recv.at[3], device_id={"tp": 1 - tp}, device_id_type=MESH
        )

    loads = [
        pltpu.make_async_copy(later_hbm, xin.at[0], load_sem.at[0]),
        pltpu.make_async_copy(earlier_hbm, xin.at[1], load_sem.at[1]),
        pltpu.make_async_copy(cot_hbm, cot, load_sem.at[2]),
        pltpu.make_async_copy(grun_hbm, run.at[0], load_sem.at[3]),
        pltpu.make_async_copy(urun_hbm, run.at[1], load_sem.at[4]),
    ]

    def shard_loads(j):
        columns = pl.ds(pl.multiple_of(j * HALF, HALF), HALF)
        mine = (j, own["z"], own["y"], own["x"], ALL)
        return [
            pltpu.make_async_copy(gw_hbm.at[:, columns], w.at[(*mine, pl.ds(0, HALF))], w_sem.at[0, j]),
            pltpu.make_async_copy(uw_hbm.at[:, columns], w.at[(*mine, pl.ds(HALF, HALF))], w_sem.at[1, j]),
        ]

    @pl.loop(0, blocks)
    def _(j):
        for c in shard_loads(j):
            c.start()

    for c in loads:
        c.start()

    barrier = pltpu.get_barrier_semaphore()
    greeted = [peer(a, by) for a in "xyz" for by in (1, 2, 3)] + [{"tp": 1 - tp}]
    for device in greeted:
        pl.semaphore_signal(barrier, inc=1, device_id=device, device_id_type=MESH)
    pl.semaphore_wait(barrier, len(greeted))

    @pl.loop(0, blocks)
    def _(j):
        for c in shard_loads(j):
            c.wait()

    step_rows = 32 if rows % 32 == 0 else rows

    def normalize():
        for c in loads:
            c.wait()

        @pl.loop(0, rows // step_rows)
        def _(i):
            at = pl.ds(pl.multiple_of(i * step_rows, step_rows), step_rows)
            for m, out in ((0, xl), (1, xe)):
                values = xin[m, at, :].astype(F32)
                inv = lax.rsqrt(jnp.mean(values * values, axis=1, keepdims=True) + EPSILON)
                out[tp, at, :] = (values * inv * gain_ref[...]).astype(BF16)
                if m == 1:
                    inv_ref[at, :] = inv

        tp_copy(0, xl.at[tp]).start()
        tp_copy(1, xe.at[tp]).start()
        slab = min(256, width)

        @pl.loop(0, width // slab)
        def _(i):
            at = pl.ds(pl.multiple_of(i * slab, slab), slab)
            xt[tp, at, :] = xe[tp, :, at].T

        tp_copy(2, xt.at[tp]).start()
        acc[...] = jnp.zeros_like(acc)

    def exchanged():
        for i, ref in ((0, xl), (1, xe), (2, xt)):
            tp_copy(i, ref.at[tp]).wait_send()
            tp_received(i, ref.at[1 - tp]).wait_recv()

    def block_weight(j):
        return w[j].reshape(width, 2 * HALF)

    def backward(j):
        columns = pl.ds(pl.multiple_of(j * HALF, HALF), HALF)

        @pl.loop(0, 2)
        def _(m):
            both = jnp.dot(xe[m], block_weight(j), preferred_element_type=F32)
            gate, up = both[:, :HALF], both[:, HALF:]
            s = sigmoid(gate)
            c = cot[pl.ds(pl.multiple_of(m * rows, rows), rows), columns].astype(F32)
            d[m, :, 0:HALF] = (c * up * s * (1.0 + gate * (1.0 - s))).astype(BF16)
            d[m, :, HALF:] = (c * gate * s).astype(BF16)

        @pl.loop(0, 4)
        def _(k):
            z, y = k // 2, 2 * (k % 2)
            at = pl.ds(pl.multiple_of(k * (width // 4), width // 4), width // 4)
            part = jnp.dot(xt[0, at, :], d[0], preferred_element_type=F32)
            part = part + jnp.dot(xt[1, at, :], d[1], preferred_element_type=F32)
            g[j, z, pl.ds(y, 2)] = part.astype(BF16).reshape(2, 4, 4 * quarter, 2 * HALF)

    def later(j):
        @pl.loop(0, 2)
        def _(m):
            both = jnp.dot(xl[m], block_weight(j), preferred_element_type=F32)
            gate, up = both[:, :HALF], both[:, HALF:]
            lh[j, pl.ds(pl.multiple_of(m * rows, rows), rows), :] = (gate * sigmoid(gate) * up).astype(BF16)

        hidden_copy(j).start()

    def hidden_copy(j):
        columns = pl.ds(pl.multiple_of(j * HALF, HALF), HALF)
        return pltpu.make_async_copy(lh.at[j], hidden_hbm.at[:, columns], out_sem.at[j])

    def input_gradient(j):
        @pl.loop(0, 4)
        def _(k):
            z, y = k // 2, 2 * (k % 2)
            at = pl.ds(pl.multiple_of(k * (width // 4), width // 4), width // 4)
            part = w[j, z, pl.ds(y, 2)].reshape(width // 4, 2 * HALF)
            for m in range(2):
                acc[m, :, at] = acc[m, :, at] + lax.dot_general(
                    d[m], part, (((1,), (1,)), ((), ())), preferred_element_type=F32
                )

    def send_input_gradient():
        @pl.loop(0, rows // step_rows)
        def _(i):
            at = pl.ds(pl.multiple_of(i * step_rows, step_rows), step_rows)
            dn[0, at, :] = acc[tp, at, :].astype(BF16)
            dn[1, at, :] = acc[1 - tp, at, :].astype(BF16)

        dn_copy().start()

    def finish_input_gradient():
        dn_copy().wait()
        gain = gain_ref[...]
        own_slot = gbuf.at[0, own["x"]]
        own_slot[...] = jnp.zeros_like(own_slot)

        @pl.loop(0, rows // step_rows)
        def _(i):
            at = pl.ds(pl.multiple_of(i * step_rows, step_rows), step_rows)
            d_norm = dn[0, at, :].astype(F32) + dn[2, at, :].astype(F32)
            values = xin[1, at, :].astype(F32)
            inv = inv_ref[at, :]
            scaled = d_norm * gain
            inner = jnp.mean(scaled * values, axis=1, keepdims=True)
            dn[1, at, :] = (inv * scaled - values * (inv * inv * inv) * inner).astype(BF16)
            own_slot[...] = own_slot[...] + jnp.sum(d_norm * values * inv, axis=0, keepdims=True)

        grad_copy().start()

    def grad_copy():
        return pltpu.make_async_copy(dn.at[1], grad_hbm, out_sem.at[blocks])

    def gain_copies(r):
        axis = ("x", "y", "z")[r]
        at = (own["x"], own["y"], ring_z)[r]
        return [
            pltpu.make_async_remote_copy(
                src_ref=gbuf.at[r, at], dst_ref=gbuf.at[r, at], send_sem=gain_send.at[r, k], recv_sem=gain_recv.at[r, k],
                device_id=peer(axis, k), device_id_type=MESH,
            )
            for k in (1, 2, 3)
        ]

    def gain_received(r):
        axis = ("x", "y", "z")[r]
        at = (own["x"], own["y"], ring_z)[r]
        return [
            pltpu.make_async_remote_copy(
                src_ref=gbuf.at[r, at], dst_ref=gbuf.at[r, (at - k) % 4], send_sem=gain_send.at[r, k], recv_sem=gain_recv.at[r, k],
                device_id=peer(axis, k), device_id_type=MESH,
            )
            for k in (1, 2, 3)
        ]

    def gain_sum(r):
        for c in gain_received(r):
            c.wait()
        return (gbuf[r, 0] + gbuf[r, 1]) + (gbuf[r, 2] + gbuf[r, 3])

    def gain_tp():
        return pltpu.make_async_remote_copy(
            src_ref=gbuf.at[3, 0], dst_ref=gbuf.at[3, 1], send_sem=gain_send.at[3, 1], recv_sem=gain_recv.at[3, 1],
            device_id={"tp": 1 - tp}, device_id_type=MESH,
        )

    def gain_step(r):
        if r == 0:
            finish_input_gradient()
            for c in gain_copies(0):
                c.start()
        elif r < 3:
            gbuf[r, (own["x"], own["y"], ring_z)[r]] = gain_sum(r - 1)
            for c in gain_copies(r):
                c.start()
        elif r == 3:
            gbuf[3, 0] = gain_sum(2)
            gain_tp().start()
        else:
            gain_tp().wait()
            gain_tot[...] = gain_run[...] + factor * (gbuf[3, 0] + gbuf[3, 1])

    last = 5 + blocks - 1

    @pl.loop(0, last + 8)
    def _(t):
        def at_stage(offset, run_stage):
            j = t - offset

            @pl.when((j >= 0) & (j < blocks))
            def _():
                run_stage(j)

        for s in (1, 2, 3, 4, 0):
            at_stage(s, functools.partial(ag_stage, s=s))
        for s in (1, 2, 3, 4, 5):
            at_stage(5 + s, functools.partial(rs_stage, s=s))
        at_stage(11, rs_finish)

        @pl.when(t == 0)
        def _():
            normalize()

        @pl.when(t == 4)
        def _():
            exchanged()

        def compute(j):
            ag_stage(j, 5)
            backward(j)
            rs_stage(j, 0)
            later(j)
            input_gradient(j)

        at_stage(5, compute)

        @pl.when(t == last)
        def _():
            send_input_gradient()

        for r in range(5):
            @pl.when(t == last + 1 + r)
            def _():
                gain_step(r)

    outs = [pltpu.make_async_copy(run.at[0], gtot_hbm, load_sem.at[0]), pltpu.make_async_copy(run.at[1], utot_hbm, load_sem.at[1])]
    for c in outs:
        c.start()

    @pl.loop(0, blocks)
    def _(j):
        hidden_copy(j).wait()

    grad_copy().wait()
    for c in outs:
        c.wait()


def body(later_input, earlier_input, hidden_cot, norm_gain, gate_weight, up_weight, gate_running, up_running, gain_running):
    rows, width = later_input.shape
    shard, hidden = gate_weight.shape
    blocks = hidden // HALF
    quarter = shard // 4
    tokens = rows * lax.axis_size("rep") * lax.axis_size("fs") * lax.axis_size("tp")
    factor = 1.0 / math.sqrt(tokens)
    whole = (blocks, 2, 4, 4, shard, 2 * HALF)
    hbm = pl.BlockSpec(memory_space=pl.ANY)
    vmem = pl.BlockSpec(memory_space=pltpu.VMEM)
    dma = pltpu.SemaphoreType.DMA
    out = pl.pallas_call(
        functools.partial(kernel, blocks, factor),
        out_shape=(
            jax.ShapeDtypeStruct((2 * rows, hidden), BF16),
            jax.ShapeDtypeStruct((rows, width), BF16),
            jax.ShapeDtypeStruct((shard, hidden), F32),
            jax.ShapeDtypeStruct((shard, hidden), F32),
            jax.ShapeDtypeStruct((1, width), F32),
        ),
        in_specs=[hbm, hbm, hbm, vmem, hbm, hbm, hbm, hbm, vmem],
        out_specs=(hbm, hbm, hbm, hbm, vmem),
        scratch_shapes=[
            pltpu.VMEM(whole, BF16),
            pltpu.VMEM(whole, BF16),
            pltpu.VMEM((2, rows, width), BF16),
            pltpu.VMEM((2, rows, width), BF16),
            pltpu.VMEM((2, rows, width), BF16),
            pltpu.VMEM((2, width, rows), BF16),
            pltpu.VMEM((2 * rows, hidden), BF16),
            pltpu.VMEM((2, rows, 2 * HALF), BF16),
            pltpu.VMEM((2, rows, width), F32),
            pltpu.VMEM((blocks, 2 * rows, HALF), BF16),
            pltpu.VMEM((3, rows, width), BF16),
            pltpu.VMEM((rows, 1), F32),
            pltpu.VMEM((2, shard, hidden), F32),
            pltpu.VMEM((4, 4, 1, width), F32),
            pltpu.VMEM((blocks, shard, 2 * HALF), BF16),
            *[pltpu.VMEM(s, BF16) for s in landing_shapes(blocks, quarter)],
            dma((blocks, 40)),
            dma((blocks, 40)),
            dma((blocks, 41)),
            dma((blocks, 41)),
            dma((5,)),
            dma((2, blocks)),
            dma((4,)),
            dma((4,)),
            dma((2, 4, 4)),
            dma((blocks + 1,)),
        ],
        compiler_params=pltpu.CompilerParams(collective_id=0, has_side_effects=True, vmem_limit_bytes=67043328),
        cost_estimate=pl.CostEstimate(flops=16 * rows * width * hidden * 2, bytes_accessed=16 << 20, transcendentals=0),
        name="half_step",
    )(
        later_input, earlier_input, hidden_cot, norm_gain.reshape(1, width), gate_weight, up_weight, gate_running, up_running,
        gain_running.reshape(1, width),
    )
    hidden_out, grad, gate_total, up_total, gain_total = out
    return hidden_out, grad, gate_total, up_total, gain_total.reshape(width)


def solution(mesh):
    in_specs = (
        P(("rep", "fs", "tp"), None),
        P(("rep", "fs", "tp"), None),
        P(("rep", "fs"), "tp"),
        P(),
        P("fs", "tp"),
        P("fs", "tp"),
        P("fs", "tp"),
        P("fs", "tp"),
        P(),
    )
    out_specs = (
        P(("rep", "fs"), "tp"),
        P(("rep", "fs", "tp"), None),
        P("fs", "tp"),
        P("fs", "tp"),
        P(),
    )
    return jax.shard_map(body, mesh=mesh, in_specs=in_specs, out_specs=out_specs, check_vma=False)
```

```python
import functools
import math

import jax
import jax.numpy as jnp
from jax import lax
from jax.experimental import pallas as pl
from jax.experimental.pallas import tpu as pltpu
from jax.sharding import PartitionSpec as P

EPSILON = 1e-06
MESH = pl.DeviceIdType.MESH
HALF = 128
F32, BF16 = jnp.float32, jnp.bfloat16
SIZE = {"z": 2, "y": 4, "x": 4}
ORDERS = (("y", "z", "x"), ("x", "z", "y"), ("x", "y", "z"), ("y", "x", "z"))
ALL = slice(None)
AG_SHARDS = (2, 1, 6, 10, 12)
RS_SHARDS = (12, 10, 6, 1, 2)


def sigmoid(v):
    return 1.0 / (1.0 + jnp.exp(-v))


def landing_shapes(blocks, quarter):
    shapes = []
    for order in ORDERS:
        full = [a for a in "zyx"]
        for axis in reversed(order):
            full.remove(axis)
            lead = tuple(SIZE[a] for a in full)
            if axis == "z":
                shapes.append((blocks, 2, *lead, quarter, HALF))
            else:
                shapes.append((blocks, 2, *lead, quarter, HALF))
                shapes.append((blocks, 2, *lead, quarter, 2 * HALF))
    return shapes


def kernel(
    blocks, factor, later_hbm, earlier_hbm, cot_hbm, gain_ref, gw_hbm, uw_hbm, grun_hbm, urun_hbm, gain_run,
    hidden_hbm, grad_hbm, gtot_hbm, utot_hbm, gain_tot,
    w, g, xin, xl, xe, xt, cot, d, acc, lh, dn, inv_ref, run, gbuf, rep_in, *rest,
):
    landing = list(rest[:-10])
    ag_send, ag_recv, rs_send, rs_recv, load_sem, w_sem, tp_send, tp_recv, gs, out_sem = rest[-10:]
    gain_send, gain_recv = gs.at[0], gs.at[1]
    rows = xin.shape[1]
    width = xin.shape[2]
    quarter = g.shape[4] // 4
    rep, fs, tp = lax.axis_index("rep"), lax.axis_index("fs"), lax.axis_index("tp")
    own = {"x": fs % 4, "y": (fs // 4) % 4, "z": fs // 16}
    ring_z = 2 * rep + own["z"]

    def peer(axis, by):
        if axis == "z":
            z = (ring_z + by) % 4
            return {"rep": z // 2, "fs": (z % 2) * 16 + own["y"] * 4 + own["x"]}
        c = (own[axis] + by) % 4
        if axis == "y":
            return {"fs": own["z"] * 16 + c * 4 + own["x"]}
        return {"fs": own["z"] * 16 + own["y"] * 4 + c}

    def shifted(axis, by):
        return (1 - own["z"] if by else own["z"]) if axis == "z" else (own[axis] + by) % 4

    HALVES = (pl.ds(0, HALF), pl.ds(HALF, HALF), pl.ds(0, 2 * HALF))

    def region(j, q, sel, half):
        return (j, sel["z"], sel["y"], sel["x"], pl.ds(q * quarter, quarter), HALVES[half])

    def sel_of(full, axis, coordinate):
        s = {a: (ALL if a in full else own[a]) for a in "zyx"}
        s[axis] = coordinate
        return s

    ag_plan = []
    count = 0
    for q, order in enumerate(ORDERS):
        phases = []
        for p, axis in enumerate(order):
            full = order[:p]
            if axis == "z":
                group = []
                for k, by in enumerate((1, -1)):
                    group.append((count, (q, sel_of(full, "z", own["z"]), k), ("z", by), (q, sel_of(full, "z", 1 - own["z"]), k)))
                    count += 1
                phases.append(("z", [group]))
            else:
                first, second = [], []
                for k, by in enumerate((1, -1)):
                    first.append((count, (q, sel_of(full, axis, own[axis]), 2), (axis, by), (q, sel_of(full, axis, shifted(axis, -by)), 2)))
                    count += 1
                for k, by in enumerate((1, -1)):
                    second.append((count, (q, sel_of(full, axis, shifted(axis, -by)), k), (axis, by), (q, sel_of(full, axis, shifted(axis, 2)), k)))
                    count += 1
                phases.append((axis, [first, second]))
        ag_plan.append([group for _, groups in phases for group in groups])

    def shards(n):
        if n <= 4:
            return w.at[0, 0, 0, pl.ds(0, n)]
        if n % 4 == 0:
            return w.at[0, 0, pl.ds(0, n // 4)]
        return w.at[pl.ds(0, n // 2), :, 0, 0]

    def await_stage(n, send, recv):
        pltpu.make_async_copy(shards(n), shards(n), send).wait()
        pltpu.make_async_copy(shards(n), shards(n), recv).wait()

    def ag_start(j, s, t):
        _, src, to, _ = t
        pltpu.make_async_remote_copy(
            src_ref=w.at[region(j, *src)], dst_ref=w.at[region(j, *src)], send_sem=ag_send.at[s], recv_sem=ag_recv.at[j % 2, s],
            device_id=peer(*to), device_id_type=MESH,
        ).start()

    def ag_stage(j, s):
        if s >= 1:
            await_stage(AG_SHARDS[s - 1], ag_send.at[s - 1], ag_recv.at[j % 2, s - 1])
        if s < 5:
            for plan in ag_plan:
                for t in plan[s]:
                    ag_start(j, s, t)

    rs_plan = []
    count, place = 0, 0
    for q, order in enumerate(ORDERS):
        groups = []
        full = ["z", "y", "x"]
        for axis in reversed(order):
            full.remove(axis)
            if axis == "z":
                group = []
                for k, by in enumerate((1, -1)):
                    group.append((count, (q, sel_of(full, "z", 1 - own["z"]), k), ("z", by), place, k, (q, sel_of(full, "z", own["z"]), k)))
                    count += 1
                groups.append(group)
                place += 1
            else:
                first, second = [], []
                for k, by in enumerate((1, -1)):
                    first.append((count, (q, sel_of(full, axis, shifted(axis, 2)), k), (axis, by), place, k, (q, sel_of(full, axis, shifted(axis, by)), k)))
                    count += 1
                for k, by in enumerate((1, -1)):
                    second.append((count, (q, sel_of(full, axis, shifted(axis, by)), 2), (axis, by), place + 1, k, (q, sel_of(full, axis, own[axis]), 2)))
                    count += 1
                groups += [first, second]
                place += 2
        rs_plan.append(groups)

    def rs_start(j, s, t):
        _, src, to, at, slot, _ = t
        pltpu.make_async_remote_copy(
            src_ref=g.at[region(j, *src)], dst_ref=landing[at].at[j, slot], send_sem=rs_send.at[s], recv_sem=rs_recv.at[j % 2, s],
            device_id=peer(*to), device_id_type=MESH,
        ).start()

    def rep_copy(j):
        return pltpu.make_async_remote_copy(
            src_ref=g.at[j, own["z"], own["y"], own["x"]], dst_ref=rep_in.at[j], send_sem=rs_send.at[5],
            recv_sem=rs_recv.at[j % 2, 5], device_id=peer("z", 2), device_id_type=MESH,
        )

    def rs_stage(j, s):
        if s >= 1:
            await_stage(RS_SHARDS[s - 1], rs_send.at[s - 1], rs_recv.at[j % 2, s - 1])
        for plan in rs_plan:
            if s >= 1:
                for _, _, _, at, slot, target in plan[s - 1]:
                    to = region(j, *target)
                    g[to] = (g[to].astype(F32) + landing[at][j, slot].astype(F32)).astype(BF16)
            if s < 5:
                for t in plan[s]:
                    rs_start(j, s, t)
        if s == 5:
            rep_copy(j).start()

    def rs_finish(j):
        rep_copy(j).wait()
        total = g[j, own["z"], own["y"], own["x"]].astype(F32) + rep_in[j].astype(F32)
        columns = pl.ds(pl.multiple_of(j * HALF, HALF), HALF)
        run[0, :, columns] = run[0, :, columns] + factor * total[:, :HALF]
        run[1, :, columns] = run[1, :, columns] + factor * total[:, HALF:]

    def tp_copy(i, ref):
        return pltpu.make_async_remote_copy(
            src_ref=ref, dst_ref=ref, send_sem=tp_send.at[i], recv_sem=tp_recv.at[i], device_id={"tp": 1 - tp}, device_id_type=MESH
        )

    def tp_received(i, ref):
        return pltpu.make_async_remote_copy(
            src_ref=ref, dst_ref=ref, send_sem=tp_send.at[i], recv_sem=tp_recv.at[i], device_id={"tp": 1 - tp}, device_id_type=MESH
        )

    def dn_copy():
        return pltpu.make_async_remote_copy(
            src_ref=dn.at[1], dst_ref=dn.at[2], send_sem=tp_send.at[3], recv_sem=tp_recv.at[3], device_id={"tp": 1 - tp}, device_id_type=MESH
        )

    loads = [
        pltpu.make_async_copy(later_hbm, xin.at[0], load_sem.at[0]),
        pltpu.make_async_copy(earlier_hbm, xin.at[1], load_sem.at[1]),
        pltpu.make_async_copy(cot_hbm, cot, load_sem.at[2]),
        pltpu.make_async_copy(grun_hbm, run.at[0], load_sem.at[3]),
        pltpu.make_async_copy(urun_hbm, run.at[1], load_sem.at[4]),
    ]

    def shard_loads(j):
        columns = pl.ds(pl.multiple_of(j * HALF, HALF), HALF)
        mine = (j, own["z"], own["y"], own["x"], ALL)
        return [
            pltpu.make_async_copy(gw_hbm.at[:, columns], w.at[(*mine, pl.ds(0, HALF))], w_sem.at[0, j]),
            pltpu.make_async_copy(uw_hbm.at[:, columns], w.at[(*mine, pl.ds(HALF, HALF))], w_sem.at[1, j]),
        ]

    @pl.loop(0, blocks)
    def _(j):
        for c in shard_loads(j):
            c.start()

    for c in loads:
        c.start()

    barrier = pltpu.get_barrier_semaphore()
    greeted = [peer(a, by) for a in "xyz" for by in (1, 2, 3)] + [{"tp": 1 - tp}]
    for device in greeted:
        pl.semaphore_signal(barrier, inc=1, device_id=device, device_id_type=MESH)
    pl.semaphore_wait(barrier, len(greeted))

    @pl.loop(0, blocks)
    def _(j):
        for c in shard_loads(j):
            c.wait()

    step_rows = 32 if rows % 32 == 0 else rows

    def normalize(m, out):
        @pl.loop(0, rows // step_rows)
        def _(i):
            at = pl.ds(pl.multiple_of(i * step_rows, step_rows), step_rows)
            values = xin[m, at, :].astype(F32)
            inv = lax.rsqrt(jnp.mean(values * values, axis=1, keepdims=True) + EPSILON)
            out[tp, at, :] = (values * inv * gain_ref[...]).astype(BF16)
            if m == 1:
                inv_ref[at, :] = inv

    def prepare(t):
        if t == 0:
            for c in loads:
                c.wait()
            normalize(1, xe)
            tp_copy(1, xe.at[tp]).start()
        elif t == 1:
            slab = min(256, width)

            @pl.loop(0, width // slab)
            def _(i):
                at = pl.ds(pl.multiple_of(i * slab, slab), slab)
                xt[tp, at, :] = xe[tp, :, at].T

            tp_copy(2, xt.at[tp]).start()
        elif t == 2:
            normalize(0, xl)
            tp_copy(0, xl.at[tp]).start()
        elif t == 3:
            acc[...] = jnp.zeros_like(acc)
        else:
            exchanged()

    def exchanged():
        for i, ref in ((0, xl), (1, xe), (2, xt)):
            tp_copy(i, ref.at[tp]).wait_send()
            tp_received(i, ref.at[1 - tp]).wait_recv()

    def block_weight(j):
        return w[j].reshape(width, 2 * HALF)

    def backward(j):
        columns = pl.ds(pl.multiple_of(j * HALF, HALF), HALF)

        @pl.loop(0, 2)
        def _(m):
            both = jnp.dot(xe[m], block_weight(j), preferred_element_type=F32)
            gate, up = both[:, :HALF], both[:, HALF:]
            s = sigmoid(gate)
            c = cot[pl.ds(pl.multiple_of(m * rows, rows), rows), columns].astype(F32)
            d[m, :, 0:HALF] = (c * up * s * (1.0 + gate * (1.0 - s))).astype(BF16)
            d[m, :, HALF:] = (c * gate * s).astype(BF16)

        @pl.loop(0, 4)
        def _(k):
            z, y = k // 2, 2 * (k % 2)
            at = pl.ds(pl.multiple_of(k * (width // 4), width // 4), width // 4)
            part = jnp.dot(xt[0, at, :], d[0], preferred_element_type=F32)
            part = part + jnp.dot(xt[1, at, :], d[1], preferred_element_type=F32)
            g[j, z, pl.ds(y, 2)] = part.astype(BF16).reshape(2, 4, 4 * quarter, 2 * HALF)

    def later(j):
        @pl.loop(0, 2)
        def _(m):
            both = jnp.dot(xl[m], block_weight(j), preferred_element_type=F32)
            gate, up = both[:, :HALF], both[:, HALF:]
            lh[j, pl.ds(pl.multiple_of(m * rows, rows), rows), :] = (gate * sigmoid(gate) * up).astype(BF16)

        hidden_copy(j).start()

    def hidden_copy(j):
        columns = pl.ds(pl.multiple_of(j * HALF, HALF), HALF)
        return pltpu.make_async_copy(lh.at[j], hidden_hbm.at[:, columns], out_sem.at[j])

    def input_gradient(j):
        @pl.loop(0, 4)
        def _(k):
            z, y = k // 2, 2 * (k % 2)
            at = pl.ds(pl.multiple_of(k * (width // 4), width // 4), width // 4)
            part = w[j, z, pl.ds(y, 2)].reshape(width // 4, 2 * HALF)
            for m in range(2):
                acc[m, :, at] = acc[m, :, at] + lax.dot_general(
                    d[m], part, (((1,), (1,)), ((), ())), preferred_element_type=F32
                )

    def send_input_gradient():
        @pl.loop(0, rows // step_rows)
        def _(i):
            at = pl.ds(pl.multiple_of(i * step_rows, step_rows), step_rows)
            dn[0, at, :] = acc[tp, at, :].astype(BF16)
            dn[1, at, :] = acc[1 - tp, at, :].astype(BF16)

        dn_copy().start()

    def finish_input_gradient():
        dn_copy().wait()
        gain = gain_ref[...]
        own_slot = gbuf.at[0, own["x"]]
        own_slot[...] = jnp.zeros_like(own_slot)

        @pl.loop(0, rows // step_rows)
        def _(i):
            at = pl.ds(pl.multiple_of(i * step_rows, step_rows), step_rows)
            d_norm = dn[0, at, :].astype(F32) + dn[2, at, :].astype(F32)
            values = xin[1, at, :].astype(F32)
            inv = inv_ref[at, :]
            scaled = d_norm * gain
            inner = jnp.mean(scaled * values, axis=1, keepdims=True)
            dn[1, at, :] = (inv * scaled - values * (inv * inv * inv) * inner).astype(BF16)
            own_slot[...] = own_slot[...] + jnp.sum(d_norm * values * inv, axis=0, keepdims=True)

        grad_copy().start()

    def grad_copy():
        return pltpu.make_async_copy(dn.at[1], grad_hbm, out_sem.at[blocks])

    def gain_copies(r):
        axis = ("x", "y", "z")[r]
        at = (own["x"], own["y"], ring_z)[r]
        return [
            pltpu.make_async_remote_copy(
                src_ref=gbuf.at[r, at], dst_ref=gbuf.at[r, at], send_sem=gain_send.at[r, k], recv_sem=gain_recv.at[r, k],
                device_id=peer(axis, k), device_id_type=MESH,
            )
            for k in (1, 2, 3)
        ]

    def gain_received(r):
        axis = ("x", "y", "z")[r]
        at = (own["x"], own["y"], ring_z)[r]
        return [
            pltpu.make_async_remote_copy(
                src_ref=gbuf.at[r, at], dst_ref=gbuf.at[r, (at - k) % 4], send_sem=gain_send.at[r, k], recv_sem=gain_recv.at[r, k],
                device_id=peer(axis, k), device_id_type=MESH,
            )
            for k in (1, 2, 3)
        ]

    def gain_sum(r):
        for c in gain_received(r):
            c.wait()
        return (gbuf[r, 0] + gbuf[r, 1]) + (gbuf[r, 2] + gbuf[r, 3])

    def gain_tp():
        return pltpu.make_async_remote_copy(
            src_ref=gbuf.at[3, 0], dst_ref=gbuf.at[3, 1], send_sem=gain_send.at[3, 1], recv_sem=gain_recv.at[3, 1],
            device_id={"tp": 1 - tp}, device_id_type=MESH,
        )

    def gain_step(r):
        if r == 0:
            finish_input_gradient()
            for c in gain_copies(0):
                c.start()
        elif r < 3:
            gbuf[r, (own["x"], own["y"], ring_z)[r]] = gain_sum(r - 1)
            for c in gain_copies(r):
                c.start()
        elif r == 3:
            gbuf[3, 0] = gain_sum(2)
            gain_tp().start()
        else:
            gain_tp().wait()
            gain_tot[...] = gain_run[...] + factor * (gbuf[3, 0] + gbuf[3, 1])

    last = 5 + blocks - 1

    @pl.loop(0, last + 8)
    def _(t):
        def at_stage(offset, run_stage):
            j = t - offset

            @pl.when((j >= 0) & (j < blocks))
            def _():
                run_stage(j)

        for s in (5, 4, 3, 2, 1, 0):
            at_stage(s, functools.partial(ag_stage, s=s))
        at_stage(11, rs_finish)
        for s in (5, 4, 3, 2, 1):
            at_stage(5 + s, functools.partial(rs_stage, s=s))

        for k in range(5):
            @pl.when(t == k)
            def _():
                prepare(k)

        def compute(j):
            backward(j)
            rs_stage(j, 0)
            later(j)
            input_gradient(j)

        at_stage(5, compute)

        @pl.when(t == last)
        def _():
            send_input_gradient()

        for r in range(5):
            @pl.when(t == last + 1 + r)
            def _():
                gain_step(r)

    outs = [pltpu.make_async_copy(run.at[0], gtot_hbm, load_sem.at[0]), pltpu.make_async_copy(run.at[1], utot_hbm, load_sem.at[1])]
    for c in outs:
        c.start()

    @pl.loop(0, blocks)
    def _(j):
        hidden_copy(j).wait()

    grad_copy().wait()
    for c in outs:
        c.wait()


def body(later_input, earlier_input, hidden_cot, norm_gain, gate_weight, up_weight, gate_running, up_running, gain_running):
    rows, width = later_input.shape
    shard, hidden = gate_weight.shape
    blocks = hidden // HALF
    quarter = shard // 4
    tokens = rows * lax.axis_size("rep") * lax.axis_size("fs") * lax.axis_size("tp")
    factor = 1.0 / math.sqrt(tokens)
    whole = (blocks, 2, 4, 4, shard, 2 * HALF)
    hbm = pl.BlockSpec(memory_space=pl.ANY)
    vmem = pl.BlockSpec(memory_space=pltpu.VMEM)
    dma = pltpu.SemaphoreType.DMA
    out = pl.pallas_call(
        functools.partial(kernel, blocks, factor),
        out_shape=(
            jax.ShapeDtypeStruct((2 * rows, hidden), BF16),
            jax.ShapeDtypeStruct((rows, width), BF16),
            jax.ShapeDtypeStruct((shard, hidden), F32),
            jax.ShapeDtypeStruct((shard, hidden), F32),
            jax.ShapeDtypeStruct((1, width), F32),
        ),
        in_specs=[hbm, hbm, hbm, vmem, hbm, hbm, hbm, hbm, vmem],
        out_specs=(hbm, hbm, hbm, hbm, vmem),
        scratch_shapes=[
            pltpu.VMEM(whole, BF16),
            pltpu.VMEM(whole, BF16),
            pltpu.VMEM((2, rows, width), BF16),
            pltpu.VMEM((2, rows, width), BF16),
            pltpu.VMEM((2, rows, width), BF16),
            pltpu.VMEM((2, width, rows), BF16),
            pltpu.VMEM((2 * rows, hidden), BF16),
            pltpu.VMEM((2, rows, 2 * HALF), BF16),
            pltpu.VMEM((2, rows, width), F32),
            pltpu.VMEM((blocks, 2 * rows, HALF), BF16),
            pltpu.VMEM((3, rows, width), BF16),
            pltpu.VMEM((rows, 1), F32),
            pltpu.VMEM((2, shard, hidden), F32),
            pltpu.VMEM((4, 4, 1, width), F32),
            pltpu.VMEM((blocks, shard, 2 * HALF), BF16),
            *[pltpu.VMEM(s, BF16) for s in landing_shapes(blocks, quarter)],
            dma((5,)),
            dma((2, 5)),
            dma((6,)),
            dma((2, 6)),
            dma((5,)),
            dma((2, blocks)),
            dma((4,)),
            dma((4,)),
            dma((2, 4, 4)),
            dma((blocks + 1,)),
        ],
        compiler_params=pltpu.CompilerParams(collective_id=0, has_side_effects=True, vmem_limit_bytes=67043328),
        cost_estimate=pl.CostEstimate(flops=16 * rows * width * hidden * 2, bytes_accessed=16 << 20, transcendentals=0),
        name="half_step",
    )(
        later_input, earlier_input, hidden_cot, norm_gain.reshape(1, width), gate_weight, up_weight, gate_running, up_running,
        gain_running.reshape(1, width),
    )
    hidden_out, grad, gate_total, up_total, gain_total = out
    return hidden_out, grad, gate_total, up_total, gain_total.reshape(width)


def solution(mesh):
    in_specs = (
        P(("rep", "fs", "tp"), None),
        P(("rep", "fs", "tp"), None),
        P(("rep", "fs"), "tp"),
        P(),
        P("fs", "tp"),
        P("fs", "tp"),
        P("fs", "tp"),
        P("fs", "tp"),
        P(),
    )
    out_specs = (
        P(("rep", "fs"), "tp"),
        P(("rep", "fs", "tp"), None),
        P("fs", "tp"),
        P("fs", "tp"),
        P(),
    )
    return jax.shard_map(body, mesh=mesh, in_specs=in_specs, out_specs=out_specs, check_vma=False)
```

```python
import functools
import math

import jax
import jax.numpy as jnp
from jax import lax
from jax.experimental import pallas as pl
from jax.experimental.pallas import tpu as pltpu
from jax.sharding import PartitionSpec as P

EPSILON = 1e-06
MESH = pl.DeviceIdType.MESH
HALF = 128
F32, BF16 = jnp.float32, jnp.bfloat16
SIZE = {"z": 2, "y": 4, "x": 4}
ORDERS = (("y", "z", "x"), ("x", "z", "y"), ("x", "y", "z"), ("y", "x", "z"))
ALL = slice(None)
AG_SHARDS = ((1, 1), (0.5, 0.5), (2, 4), (8, 2), (4, 8))
RS_SHARDS = ((4, 8), (8, 2), (2, 4), (0.5, 0.5), (1, 1))


def sigmoid(v):
    return 1.0 / (1.0 + jnp.exp(-v))


def landing_shapes(blocks, quarter):
    shapes = []
    for order in ORDERS:
        full = [a for a in "zyx"]
        for axis in reversed(order):
            full.remove(axis)
            lead = tuple(SIZE[a] for a in full)
            if axis == "z":
                shapes.append((blocks, 2, *lead, quarter, HALF))
            else:
                shapes.append((blocks, 2, *lead, quarter, HALF))
                shapes.append((blocks, 2, *lead, quarter, 2 * HALF))
    return shapes


def kernel(
    blocks, factor, later_hbm, earlier_hbm, cot_hbm, gain_ref, gw_hbm, uw_hbm, grun_hbm, urun_hbm, gain_run,
    hidden_hbm, grad_hbm, gtot_hbm, utot_hbm, gain_tot,
    w, g, xin, xl, xe, xt, cot, d, acc, lh, dn, inv_ref, run, gbuf, rep_in, *rest,
):
    last_in, landing = rest[0], list(rest[1:-11])
    ag_send, ag_recv, rs_send, rs_recv, once, load_sem, w_sem, tp_send, tp_recv, gs, out_sem = rest[-11:]
    gain_send, gain_recv = gs.at[0], gs.at[1]
    rows = xin.shape[1]
    width = xin.shape[2]
    quarter = g.shape[4] // 4
    rep, fs, tp = lax.axis_index("rep"), lax.axis_index("fs"), lax.axis_index("tp")
    own = {"x": fs % 4, "y": (fs // 4) % 4, "z": fs // 16}
    ring_z = 2 * rep + own["z"]

    def peer(axis, by):
        if axis == "z":
            z = (ring_z + by) % 4
            return {"rep": z // 2, "fs": (z % 2) * 16 + own["y"] * 4 + own["x"]}
        c = (own[axis] + by) % 4
        if axis == "y":
            return {"fs": own["z"] * 16 + c * 4 + own["x"]}
        return {"fs": own["z"] * 16 + own["y"] * 4 + c}

    def shifted(axis, by):
        return (1 - own["z"] if by else own["z"]) if axis == "z" else (own[axis] + by) % 4

    HALVES = (pl.ds(0, HALF), pl.ds(HALF, HALF), pl.ds(0, 2 * HALF))

    def region(j, q, sel, half):
        return (j, sel["z"], sel["y"], sel["x"], pl.ds(q * quarter, quarter), HALVES[half])

    def sel_of(full, axis, coordinate):
        s = {a: (ALL if a in full else own[a]) for a in "zyx"}
        s[axis] = coordinate
        return s

    ag_plan = []
    count = 0
    for q, order in enumerate(ORDERS):
        phases = []
        for p, axis in enumerate(order):
            full = order[:p]
            if axis == "z":
                group = []
                for k, by in enumerate((1, -1)):
                    group.append((count, (q, sel_of(full, "z", own["z"]), k), ("z", by), (q, sel_of(full, "z", 1 - own["z"]), k)))
                    count += 1
                phases.append(("z", [group]))
            else:
                first, second = [], []
                for k, by in enumerate((1, -1)):
                    first.append((count, (q, sel_of(full, axis, own[axis]), 2), (axis, by), (q, sel_of(full, axis, shifted(axis, -by)), 2)))
                    count += 1
                for k, by in enumerate((1, -1)):
                    second.append((count, (q, sel_of(full, axis, shifted(axis, -by)), k), (axis, by), (q, sel_of(full, axis, shifted(axis, 2)), k)))
                    count += 1
                phases.append((axis, [first, second]))
        ag_plan.append([group for _, groups in phases for group in groups])

    def shards(n):
        if n <= 4:
            if n == 0.5:
                return w.at[0, 0, 0, 0, pl.ds(0, 2 * quarter)]
            return w.at[0, 0, 0, pl.ds(0, n)]
        if n % 4 == 0:
            return w.at[0, 0, pl.ds(0, n // 4)]
        return w.at[:, 0, 0, 0]

    def await_stage(n, send, recv):
        pltpu.make_async_copy(shards(n), shards(n), send).wait()
        pltpu.make_async_copy(shards(n), shards(n), recv).wait()

    def ag_send_to(j, src, to, send, recv):
        pltpu.make_async_remote_copy(
            src_ref=w.at[region(j, *src)], dst_ref=w.at[region(j, *src)], send_sem=send, recv_sem=recv, device_id=peer(*to), device_id_type=MESH
        ).start()

    def ag_stage(j, s, wait=True):
        for pair in (1, 0):
            if s >= 1 and wait:
                await_stage(AG_SHARDS[s - 1][pair], ag_send.at[pair, s - 1], ag_recv.at[j % 2, pair, s - 1])
            if s < 5:
                for plan in ag_plan[2 * pair : 2 * pair + 2]:
                    for _, src, to, _ in plan[s]:
                        ag_send_to(j, src, to, ag_send.at[pair, s], ag_recv.at[j % 2, pair, s])

    def ag_first():
        for q, order in enumerate(ORDERS):
            src = (q, sel_of((), order[0], own[order[0]]), 2)
            for by in (2, 1, -1):
                ag_send_to(0, src, (order[0], by), once.at[0], once.at[1])

    def ag_second(j):
        @pl.when(j == 0)
        def _():
            await_stage(3, once.at[0], once.at[1])
            ag_stage(j, 2, wait=False)

        @pl.when(j > 0)
        def _():
            ag_stage(j, 2)

    rs_plan = []
    count, place = 0, 0
    for q, order in enumerate(ORDERS):
        groups = []
        full = ["z", "y", "x"]
        for axis in reversed(order):
            full.remove(axis)
            if axis == "z":
                group = []
                for k, by in enumerate((1, -1)):
                    group.append((count, (q, sel_of(full, "z", 1 - own["z"]), k), ("z", by), place, k, (q, sel_of(full, "z", own["z"]), k)))
                    count += 1
                groups.append(group)
                place += 1
            else:
                first, second = [], []
                for k, by in enumerate((1, -1)):
                    first.append((count, (q, sel_of(full, axis, shifted(axis, 2)), k), (axis, by), place, k, (q, sel_of(full, axis, shifted(axis, by)), k)))
                    count += 1
                for k, by in enumerate((1, -1)):
                    second.append((count, (q, sel_of(full, axis, shifted(axis, by)), 2), (axis, by), place + 1, k, (q, sel_of(full, axis, own[axis]), 2)))
                    count += 1
                groups += [first, second]
                place += 2
        rs_plan.append(groups)

    def rs_start(j, s, pair, t):
        _, src, to, at, slot, _ = t
        pltpu.make_async_remote_copy(
            src_ref=g.at[region(j, *src)], dst_ref=landing[at].at[j, slot], send_sem=rs_send.at[pair, s], recv_sem=rs_recv.at[j % 2, pair, s],
            device_id=peer(*to), device_id_type=MESH,
        ).start()

    def rep_copy(j, send, recv):
        return pltpu.make_async_remote_copy(
            src_ref=g.at[j, own["z"], own["y"], own["x"]], dst_ref=rep_in.at[j], send_sem=send, recv_sem=recv,
            device_id=peer("z", 2), device_id_type=MESH,
        )

    def rep_sems(j):
        return rs_send.at[0, 5], rs_recv.at[j % 2, 0, 5]

    def rs_collect(j, s, pair):
        await_stage(RS_SHARDS[s - 1][pair], rs_send.at[pair, s - 1], rs_recv.at[j % 2, pair, s - 1])
        for plan in rs_plan[2 * pair : 2 * pair + 2]:
            for _, _, _, at, slot, target in plan[s - 1]:
                to = region(j, *target)
                g[to] = (g[to].astype(F32) + landing[at][j, slot].astype(F32)).astype(BF16)

    def rs_stage(j, s):
        for pair in (1, 0) if s in (2, 4) else (0, 1):
            if s >= 1:
                rs_collect(j, s, pair)
            if s < 5:
                for plan in rs_plan[2 * pair : 2 * pair + 2]:
                    for t in plan[s]:
                        rs_start(j, s, pair, t)
        if s == 5:
            rep_copy(j, *rep_sems(j)).start()

    def rs_last_ring(j):
        for pair in (0, 1):
            rs_collect(j, 3, pair)
            for q in (2 * pair, 2 * pair + 1):
                axis = ORDERS[q][0]
                for k, by in enumerate((2, 1, -1)):
                    pltpu.make_async_remote_copy(
                        src_ref=g.at[region(j, q, sel_of((), axis, shifted(axis, by)), 2)], dst_ref=last_in.at[q, k],
                        send_sem=once.at[2], recv_sem=once.at[3], device_id=peer(axis, by), device_id_type=MESH,
                    ).start()

    def rs_last_sum(j):
        await_stage(3, once.at[2], once.at[3])
        for q, order in enumerate(ORDERS):
            to = region(j, q, sel_of((), order[0], own[order[0]]), 2)
            g[to] = (g[to].astype(F32) + last_in[q, 0].astype(F32) + last_in[q, 1].astype(F32) + last_in[q, 2].astype(F32)).astype(BF16)
        rep_copy(j, once.at[4], once.at[5]).start()

    def choose(usual, for_last):
        def stage(j):
            if usual is not None:
                @pl.when(j < blocks - 1)
                def _():
                    usual(j)

            if for_last is not None:
                @pl.when(j == blocks - 1)
                def _():
                    for_last(j)

        return stage

    def rs_finish(j, sems=rep_sems):
        rep_copy(j, *sems(j)).wait()
        total = g[j, own["z"], own["y"], own["x"]].astype(F32) + rep_in[j].astype(F32)
        columns = pl.ds(pl.multiple_of(j * HALF, HALF), HALF)
        run[0, :, columns] = run[0, :, columns] + factor * total[:, :HALF]
        run[1, :, columns] = run[1, :, columns] + factor * total[:, HALF:]

    def tp_copy(i, ref):
        return pltpu.make_async_remote_copy(
            src_ref=ref, dst_ref=ref, send_sem=tp_send.at[i], recv_sem=tp_recv.at[i], device_id={"tp": 1 - tp}, device_id_type=MESH
        )

    def tp_received(i, ref):
        return pltpu.make_async_remote_copy(
            src_ref=ref, dst_ref=ref, send_sem=tp_send.at[i], recv_sem=tp_recv.at[i], device_id={"tp": 1 - tp}, device_id_type=MESH
        )

    def dn_copy():
        return pltpu.make_async_remote_copy(
            src_ref=dn.at[1], dst_ref=dn.at[2], send_sem=tp_send.at[3], recv_sem=tp_recv.at[3], device_id={"tp": 1 - tp}, device_id_type=MESH
        )

    loads = [
        pltpu.make_async_copy(later_hbm, xin.at[0], load_sem.at[0]),
        pltpu.make_async_copy(earlier_hbm, xin.at[1], load_sem.at[1]),
        pltpu.make_async_copy(cot_hbm, cot, load_sem.at[2]),
        pltpu.make_async_copy(grun_hbm, run.at[0], load_sem.at[3]),
        pltpu.make_async_copy(urun_hbm, run.at[1], load_sem.at[4]),
    ]

    def shard_loads(j):
        columns = pl.ds(pl.multiple_of(j * HALF, HALF), HALF)
        mine = (j, own["z"], own["y"], own["x"], ALL)
        return [
            pltpu.make_async_copy(gw_hbm.at[:, columns], w.at[(*mine, pl.ds(0, HALF))], w_sem.at[0]),
            pltpu.make_async_copy(uw_hbm.at[:, columns], w.at[(*mine, pl.ds(HALF, HALF))], w_sem.at[0]),
        ]

    @pl.loop(0, blocks)
    def _(j):
        for c in shard_loads(j):
            c.start()

    for c in loads:
        c.start()

    barrier = pltpu.get_barrier_semaphore()
    greeted = [peer(a, by) for a in "xyz" for by in (1, 2, 3)] + [{"tp": 1 - tp}]
    for device in greeted:
        pl.semaphore_signal(barrier, inc=1, device_id=device, device_id_type=MESH)
    pl.semaphore_wait(barrier, len(greeted))

    pltpu.make_async_copy(w.at[:, own["z"], own["y"], own["x"]], w.at[:, own["z"], own["y"], own["x"]], w_sem.at[0]).wait()
    ag_first()

    step_rows = 32 if rows % 32 == 0 else rows

    def normalize(m, out):
        @pl.loop(0, rows // step_rows)
        def _(i):
            at = pl.ds(pl.multiple_of(i * step_rows, step_rows), step_rows)
            values = xin[m, at, :].astype(F32)
            inv = lax.rsqrt(jnp.mean(values * values, axis=1, keepdims=True) + EPSILON)
            out[tp, at, :] = (values * inv * gain_ref[...]).astype(BF16)
            if m == 1:
                inv_ref[at, :] = inv

    def prepare(t):
        if t == 0:
            for c in loads:
                c.wait()
            normalize(1, xe)
            tp_copy(1, xe.at[tp]).start()
        elif t == 1:
            slab = min(256, width)

            @pl.loop(0, width // slab)
            def _(i):
                at = pl.ds(pl.multiple_of(i * slab, slab), slab)
                xt[tp, at, :] = xe[tp, :, at].T

            tp_copy(2, xt.at[tp]).start()
        elif t == 2:
            normalize(0, xl)
            tp_copy(0, xl.at[tp]).start()
        elif t == 3:
            acc[...] = jnp.zeros_like(acc)
        else:
            exchanged()

    def exchanged():
        for i, ref in ((0, xl), (1, xe), (2, xt)):
            tp_copy(i, ref.at[tp]).wait_send()
            tp_received(i, ref.at[1 - tp]).wait_recv()

    def block_weight(j):
        return w[j].reshape(width, 2 * HALF)

    def backward(j):
        columns = pl.ds(pl.multiple_of(j * HALF, HALF), HALF)

        @pl.loop(0, 2)
        def _(m):
            both = jnp.dot(xe[m], block_weight(j), preferred_element_type=F32)
            gate, up = both[:, :HALF], both[:, HALF:]
            s = sigmoid(gate)
            c = cot[pl.ds(pl.multiple_of(m * rows, rows), rows), columns].astype(F32)
            d[m, :, 0:HALF] = (c * up * s * (1.0 + gate * (1.0 - s))).astype(BF16)
            d[m, :, HALF:] = (c * gate * s).astype(BF16)

        @pl.loop(0, 4)
        def _(k):
            z, y = k // 2, 2 * (k % 2)
            at = pl.ds(pl.multiple_of(k * (width // 4), width // 4), width // 4)
            part = jnp.dot(xt[0, at, :], d[0], preferred_element_type=F32)
            part = part + jnp.dot(xt[1, at, :], d[1], preferred_element_type=F32)
            g[j, z, pl.ds(y, 2)] = part.astype(BF16).reshape(2, 4, 4 * quarter, 2 * HALF)

    def later(j):
        @pl.loop(0, 2)
        def _(m):
            both = jnp.dot(xl[m], block_weight(j), preferred_element_type=F32)
            gate, up = both[:, :HALF], both[:, HALF:]
            lh[j, pl.ds(pl.multiple_of(m * rows, rows), rows), :] = (gate * sigmoid(gate) * up).astype(BF16)

        hidden_copy(j).start()

    def hidden_copy(j):
        columns = pl.ds(pl.multiple_of(j * HALF, HALF), HALF)
        return pltpu.make_async_copy(lh.at[j], hidden_hbm.at[:, columns], out_sem.at[0])

    def input_gradient(j):
        @pl.loop(0, 4)
        def _(k):
            z, y = k // 2, 2 * (k % 2)
            at = pl.ds(pl.multiple_of(k * (width // 4), width // 4), width // 4)
            part = w[j, z, pl.ds(y, 2)].reshape(width // 4, 2 * HALF)
            for m in range(2):
                acc[m, :, at] = acc[m, :, at] + lax.dot_general(
                    d[m], part, (((1,), (1,)), ((), ())), preferred_element_type=F32
                )

    def send_input_gradient():
        @pl.loop(0, rows // step_rows)
        def _(i):
            at = pl.ds(pl.multiple_of(i * step_rows, step_rows), step_rows)
            dn[0, at, :] = acc[tp, at, :].astype(BF16)
            dn[1, at, :] = acc[1 - tp, at, :].astype(BF16)

        dn_copy().start()

    def finish_input_gradient():
        dn_copy().wait()
        gain = gain_ref[...]
        own_slot = gbuf.at[0, own["x"]]
        own_slot[...] = jnp.zeros_like(own_slot)

        @pl.loop(0, rows // step_rows)
        def _(i):
            at = pl.ds(pl.multiple_of(i * step_rows, step_rows), step_rows)
            d_norm = dn[0, at, :].astype(F32) + dn[2, at, :].astype(F32)
            values = xin[1, at, :].astype(F32)
            inv = inv_ref[at, :]
            scaled = d_norm * gain
            inner = jnp.mean(scaled * values, axis=1, keepdims=True)
            dn[1, at, :] = (inv * scaled - values * (inv * inv * inv) * inner).astype(BF16)
            own_slot[...] = own_slot[...] + jnp.sum(d_norm * values * inv, axis=0, keepdims=True)

        grad_copy().start()

    def grad_copy():
        return pltpu.make_async_copy(dn.at[1], grad_hbm, out_sem.at[1])

    def gain_copies(r):
        axis = ("x", "y", "z")[r]
        at = (own["x"], own["y"], ring_z)[r]
        return [
            pltpu.make_async_remote_copy(
                src_ref=gbuf.at[r, at], dst_ref=gbuf.at[r, at], send_sem=gain_send.at[3 * r + k - 1], recv_sem=gain_recv.at[3 * r + k - 1],
                device_id=peer(axis, k), device_id_type=MESH,
            )
            for k in (1, 2, 3)
        ]

    def gain_received(r):
        axis = ("x", "y", "z")[r]
        at = (own["x"], own["y"], ring_z)[r]
        return [
            pltpu.make_async_remote_copy(
                src_ref=gbuf.at[r, at], dst_ref=gbuf.at[r, (at - k) % 4], send_sem=gain_send.at[3 * r + k - 1], recv_sem=gain_recv.at[3 * r + k - 1],
                device_id=peer(axis, k), device_id_type=MESH,
            )
            for k in (1, 2, 3)
        ]

    def gain_sum(r):
        for c in gain_received(r):
            c.wait()
        return (gbuf[r, 0] + gbuf[r, 1]) + (gbuf[r, 2] + gbuf[r, 3])

    def gain_tp():
        return pltpu.make_async_remote_copy(
            src_ref=gbuf.at[3, 0], dst_ref=gbuf.at[3, 1], send_sem=gain_send.at[9], recv_sem=gain_recv.at[9],
            device_id={"tp": 1 - tp}, device_id_type=MESH,
        )

    def gain_step(r):
        if r == 0:
            finish_input_gradient()
            for c in gain_copies(0):
                c.start()
        elif r < 3:
            gbuf[r, (own["x"], own["y"], ring_z)[r]] = gain_sum(r - 1)
            for c in gain_copies(r):
                c.start()
        elif r == 3:
            gbuf[3, 0] = gain_sum(2)
            gain_tp().start()
        else:
            gain_tp().wait()
            gain_tot[...] = gain_run[...] + factor * (gbuf[3, 0] + gbuf[3, 1])

    last = 4 + blocks - 1

    @pl.loop(0, last + 6)
    def _(t):
        def at_stage(offset, run_stage):
            j = t - offset

            @pl.when((j >= 0) & (j < blocks))
            def _():
                run_stage(j)

        for s in (5, 4, 3):
            at_stage(s - 1, functools.partial(ag_stage, s=s))
        at_stage(1, ag_second)

        @pl.when((t > 0) & (t < blocks))
        def _():
            ag_stage(t, 1)

        @pl.when(t < blocks - 1)
        def _():
            ag_stage(t + 1, 0)
        for k in range(5):
            @pl.when(t == k)
            def _():
                prepare(k)

        at_stage(4, backward)
        at_stage(10, choose(rs_finish, None))
        at_stage(9, choose(functools.partial(rs_stage, s=5), lambda j: rs_finish(j, lambda _: (once.at[4], once.at[5]))))
        at_stage(8, choose(functools.partial(rs_stage, s=4), rs_last_sum))
        at_stage(7, choose(functools.partial(rs_stage, s=3), rs_last_ring))
        for s in (2, 1, 0):
            at_stage(4 + s, functools.partial(rs_stage, s=s))
        at_stage(4, later)
        at_stage(4, input_gradient)

        @pl.when(t == last)
        def _():
            send_input_gradient()

        for r in range(5):
            @pl.when(t == last + 1 + r)
            def _():
                gain_step(r)

    outs = [pltpu.make_async_copy(run.at[0], gtot_hbm, load_sem.at[0]), pltpu.make_async_copy(run.at[1], utot_hbm, load_sem.at[1])]
    for c in outs:
        c.start()

    pltpu.make_async_copy(lh, lh, out_sem.at[0]).wait()
    grad_copy().wait()
    for c in outs:
        c.wait()


def copy_kernel(*refs):
    n = (len(refs) - 2) // 3
    sources, results, held, (into, back) = refs[:n], refs[n : 2 * n], refs[2 * n : 3 * n], refs[3 * n :]
    reads = [pltpu.make_async_copy(a, b, into.at[i]) for i, (a, b) in enumerate(zip(sources, held))]
    writes = [pltpu.make_async_copy(a, b, back.at[i]) for i, (a, b) in enumerate(zip(held, results))]
    for c in reads:
        c.start()
    for a, b in zip(reads, writes):
        a.wait()
        b.start()
    for c in writes:
        c.wait()


def copied(*arrays):
    n = len(arrays)
    hbm = pl.BlockSpec(memory_space=pl.ANY)
    return pl.pallas_call(
        copy_kernel,
        out_shape=tuple(jax.ShapeDtypeStruct(a.shape, a.dtype) for a in arrays),
        in_specs=[hbm] * n,
        out_specs=(hbm,) * n,
        scratch_shapes=[*[pltpu.VMEM(a.shape, a.dtype) for a in arrays], pltpu.SemaphoreType.DMA((n,)), pltpu.SemaphoreType.DMA((n,))],
        compiler_params=pltpu.CompilerParams(vmem_limit_bytes=67043328),
        name="hand_over",
    )(*arrays)


def body(later_input, earlier_input, hidden_cot, norm_gain, gate_weight, up_weight, gate_running, up_running, gain_running):
    rows, width = later_input.shape
    shard, hidden = gate_weight.shape
    blocks = hidden // HALF
    quarter = shard // 4
    tokens = rows * lax.axis_size("rep") * lax.axis_size("fs") * lax.axis_size("tp")
    factor = 1.0 / math.sqrt(tokens)
    whole = (blocks, 2, 4, 4, shard, 2 * HALF)
    hbm = pl.BlockSpec(memory_space=pl.ANY)
    vmem = pl.BlockSpec(memory_space=pltpu.VMEM)
    dma = pltpu.SemaphoreType.DMA
    out = pl.pallas_call(
        functools.partial(kernel, blocks, factor),
        out_shape=(
            jax.ShapeDtypeStruct((2 * rows, hidden), BF16),
            jax.ShapeDtypeStruct((rows, width), BF16),
            jax.ShapeDtypeStruct((shard, hidden), F32),
            jax.ShapeDtypeStruct((shard, hidden), F32),
            jax.ShapeDtypeStruct((1, width), F32),
        ),
        in_specs=[hbm, hbm, hbm, vmem, hbm, hbm, hbm, hbm, vmem],
        out_specs=(hbm, hbm, hbm, hbm, vmem),
        scratch_shapes=[
            pltpu.VMEM(whole, BF16),
            pltpu.VMEM(whole, BF16),
            pltpu.VMEM((2, rows, width), BF16),
            pltpu.VMEM((2, rows, width), BF16),
            pltpu.VMEM((2, rows, width), BF16),
            pltpu.VMEM((2, width, rows), BF16),
            pltpu.VMEM((2 * rows, hidden), BF16),
            pltpu.VMEM((2, rows, 2 * HALF), BF16),
            pltpu.VMEM((2, rows, width), F32),
            pltpu.VMEM((blocks, 2 * rows, HALF), BF16),
            pltpu.VMEM((3, rows, width), BF16),
            pltpu.VMEM((rows, 1), F32),
            pltpu.VMEM((2, shard, hidden), F32),
            pltpu.VMEM((4, 4, 1, width), F32),
            pltpu.VMEM((blocks, shard, 2 * HALF), BF16),
            pltpu.VMEM((4, 3, quarter, 2 * HALF), BF16),
            *[pltpu.VMEM(s, BF16) for s in landing_shapes(blocks, quarter)],
            dma((2, 5)),
            dma((2, 2, 5)),
            dma((2, 6)),
            dma((2, 2, 6)),
            dma((6,)),
            dma((5,)),
            dma((1,)),
            dma((4,)),
            dma((4,)),
            dma((2, 10)),
            dma((2,)),
        ],
        compiler_params=pltpu.CompilerParams(collective_id=0, has_side_effects=True, vmem_limit_bytes=67043328),
        cost_estimate=pl.CostEstimate(flops=16 * rows * width * hidden * 2, bytes_accessed=16 << 20, transcendentals=0),
        name="half_step",
    )(
        later_input, earlier_input, hidden_cot, norm_gain.reshape(1, width), gate_weight, up_weight, gate_running, up_running,
        gain_running.reshape(1, width),
    )
    hidden_out, grad, gate_total, up_total, gain_total = copied(*out)
    return hidden_out, grad, gate_total, up_total, gain_total.reshape(width)


def solution(mesh):
    in_specs = (
        P(("rep", "fs", "tp"), None),
        P(("rep", "fs", "tp"), None),
        P(("rep", "fs"), "tp"),
        P(),
        P("fs", "tp"),
        P("fs", "tp"),
        P("fs", "tp"),
        P("fs", "tp"),
        P(),
    )
    out_specs = (
        P(("rep", "fs"), "tp"),
        P(("rep", "fs", "tp"), None),
        P("fs", "tp"),
        P("fs", "tp"),
        P(),
    )
    return jax.shard_map(body, mesh=mesh, in_specs=in_specs, out_specs=out_specs, check_vma=False)
```

```python
import functools
import math

import jax
import jax.numpy as jnp
from jax import lax
from jax.experimental import pallas as pl
from jax.experimental.pallas import tpu as pltpu
from jax.sharding import PartitionSpec as P

EPSILON = 1e-06
MESH = pl.DeviceIdType.MESH
HALF = 128
F32, BF16 = jnp.float32, jnp.bfloat16
SIZE = {"z": 2, "y": 4, "x": 4}
ORDERS = (("y", "z", "x"), ("x", "z", "y"), ("x", "y", "z"), ("y", "x", "z"))
ORDERS_MID = ORDERS[:2] + (("x", "z", "y"), ("y", "z", "x"))
ALL = slice(None)
AG_SHARDS = ((1, 1), (0.5, 0.5), (2, 4), (8, 2), (4, 8))
RS_SHARDS = ((4, 8), (8, 2), (2, 4), (0.5, 0.5), (1, 1))


def sigmoid(v):
    return 1.0 / (1.0 + jnp.exp(-v))


def landing_shapes(orders, blocks, quarter):
    shapes = []
    for order in orders:
        full = [a for a in "zyx"]
        for axis in reversed(order):
            full.remove(axis)
            lead = tuple(SIZE[a] for a in full)
            if axis == "z":
                shapes.append((blocks, 2, *lead, quarter, HALF))
            else:
                shapes.append((blocks, 2, *lead, quarter, HALF))
                shapes.append((blocks, 2, *lead, quarter, 2 * HALF))
    return shapes


def kernel(
    blocks, factor, later_hbm, earlier_hbm, cot_hbm, gain_ref, gw_hbm, uw_hbm, grun_hbm, urun_hbm, gain_run,
    hidden_hbm, grad_hbm, gtot_hbm, utot_hbm, gain_tot,
    w, g, xin, xl, xe, xt, cot, d, acc, lh, dn, inv_ref, run, gbuf, rep_in, *rest,
):
    last_in, landing = rest[0], list(rest[1:-12])
    ag_send, ag_recv, early, rs_send, rs_recv, once, load_sem, w_sem, tp_send, tp_recv, gs, out_sem = rest[-12:]
    gain_send, gain_recv = gs.at[0], gs.at[1]
    rows = xin.shape[1]
    width = xin.shape[2]
    quarter = g.shape[4] // 4
    rep, fs, tp = lax.axis_index("rep"), lax.axis_index("fs"), lax.axis_index("tp")
    own = {"x": fs % 4, "y": (fs // 4) % 4, "z": fs // 16}
    ring_z = 2 * rep + own["z"]

    def peer(axis, by):
        if axis == "z":
            z = (ring_z + by) % 4
            return {"rep": z // 2, "fs": (z % 2) * 16 + own["y"] * 4 + own["x"]}
        c = (own[axis] + by) % 4
        if axis == "y":
            return {"fs": own["z"] * 16 + c * 4 + own["x"]}
        return {"fs": own["z"] * 16 + own["y"] * 4 + c}

    def shifted(axis, by):
        return (1 - own["z"] if by else own["z"]) if axis == "z" else (own[axis] + by) % 4

    HALVES = (pl.ds(0, HALF), pl.ds(HALF, HALF), pl.ds(0, 2 * HALF))

    def region(j, q, sel, half):
        return (j, sel["z"], sel["y"], sel["x"], pl.ds(q * quarter, quarter), HALVES[half])

    def sel_of(full, axis, coordinate):
        s = {a: (ALL if a in full else own[a]) for a in "zyx"}
        s[axis] = coordinate
        return s

    def plan_gather(orders):
        plans, count = [], 0
        for q, order in enumerate(orders):
            phases = []
            for p, axis in enumerate(order):
                full = order[:p]
                if axis == "z":
                    group = []
                    for k, by in enumerate((1, -1)):
                        group.append((count, (q, sel_of(full, "z", own["z"]), k), ("z", by), (q, sel_of(full, "z", 1 - own["z"]), k)))
                        count += 1
                    phases.append(("z", [group]))
                else:
                    first, second = [], []
                    for k, by in enumerate((1, -1)):
                        first.append((count, (q, sel_of(full, axis, own[axis]), 2), (axis, by), (q, sel_of(full, axis, shifted(axis, -by)), 2)))
                        count += 1
                    for k, by in enumerate((1, -1)):
                        second.append((count, (q, sel_of(full, axis, shifted(axis, -by)), k), (axis, by), (q, sel_of(full, axis, shifted(axis, 2)), k)))
                        count += 1
                    phases.append((axis, [first, second]))
            plans.append([group for _, groups in phases for group in groups])
        return plans

    ag_plans = plan_gather(ORDERS), plan_gather(ORDERS_MID)
    ag_plan = ag_plans[0]

    def shards(n):
        if n <= 4:
            if n == 0.5:
                return w.at[0, 0, 0, 0, pl.ds(0, 2 * quarter)]
            return w.at[0, 0, 0, pl.ds(0, n)]
        if n % 4 == 0:
            return w.at[0, 0, pl.ds(0, n // 4)]
        return w.at[:, 0, 0, 0]

    def await_stage(n, send, recv):
        pltpu.make_async_copy(shards(n), shards(n), send).wait()
        pltpu.make_async_copy(shards(n), shards(n), recv).wait()

    def ag_send_to(j, src, to, send, recv):
        pltpu.make_async_remote_copy(
            src_ref=w.at[region(j, *src)], dst_ref=w.at[region(j, *src)], send_sem=send, recv_sem=recv, device_id=peer(*to), device_id_type=MESH
        ).start()

    middle = blocks // 2

    def per_kind(j, pair, run):
        if pair == 0:
            run(0)
            return

        @pl.when(j != middle)
        def _():
            run(0)

        @pl.when(j == middle)
        def _():
            run(1)

    def ag_stage(j, s, wait=True):
        for pair in (1, 0):
            def part(kind):
                if wait:
                    await_stage(AG_SHARDS[s - 1][0 if kind else pair], ag_send.at[pair + kind, s - 3], ag_recv.at[j % 3, pair + kind, s - 3])
                if s < 5:
                    for plan in ag_plans[kind][2 * pair : 2 * pair + 2]:
                        for _, src, to, _ in plan[s]:
                            ag_send_to(j, src, to, ag_send.at[pair + kind, s - 2], ag_recv.at[j % 3, pair + kind, s - 2])

            per_kind(j, pair, part)

    def ag_first():
        for q, order in enumerate(ORDERS):
            src = (q, sel_of((), order[0], own[order[0]]), 2)
            for by in (2, 1, -1):
                ag_send_to(0, src, (order[0], by), once.at[0], once.at[1])

    groups = (pl.ds(1, 1), pl.ds(2, blocks - 2))

    def ag_early(s, k):
        if s == 1:
            await_early(0, k)
        for plan in ag_plan:
            for _, src, to, _ in plan[s]:
                ag_send_to(groups[k], src, to, early.at[k, 0, s], early.at[k, 1, s])

    def await_early(s, k):
        for way in (0, 1):
            view = w.at[groups[k], 0, 0, pl.ds(0, 2)] if s == 0 else w.at[groups[k], 0, 0, 0]
            pltpu.make_async_copy(view, view, early.at[k, way, s]).wait()

    def ag_second(j):
        @pl.when(j == 0)
        def _():
            await_stage(3, once.at[0], once.at[1])

        for k in (0, 1):
            @pl.when(j == 1 + k)
            def _():
                await_early(1, k)

        ag_stage(j, 2, wait=False)

    def plan_scatter(orders, place):
        plans, count = [], 0
        for q, order in enumerate(orders):
            groups = []
            full = ["z", "y", "x"]
            for axis in reversed(order):
                full.remove(axis)
                if axis == "z":
                    group = []
                    for k, by in enumerate((1, -1)):
                        group.append((count, (q, sel_of(full, "z", 1 - own["z"]), k), ("z", by), place, k, (q, sel_of(full, "z", own["z"]), k)))
                        count += 1
                    groups.append(group)
                    place += 1
                else:
                    first, second = [], []
                    for k, by in enumerate((1, -1)):
                        first.append((count, (q, sel_of(full, axis, shifted(axis, 2)), k), (axis, by), place, k, (q, sel_of(full, axis, shifted(axis, by)), k)))
                        count += 1
                    for k, by in enumerate((1, -1)):
                        second.append((count, (q, sel_of(full, axis, shifted(axis, by)), 2), (axis, by), place + 1, k, (q, sel_of(full, axis, own[axis]), 2)))
                        count += 1
                    groups += [first, second]
                    place += 2
            plans.append(groups)
        return plans

    half_landing = len(landing) // 2
    rs_plans = plan_scatter(ORDERS, 0), plan_scatter(ORDERS_MID, half_landing)

    def land(kind, j, at, slot):
        return landing[at].at[0 if kind else j, slot]

    def rs_start(j, s, pair, kind, t):
        _, src, to, at, slot, _ = t
        pltpu.make_async_remote_copy(
            src_ref=g.at[region(j, *src)], dst_ref=land(kind, j, at, slot), send_sem=rs_send.at[pair + kind, s],
            recv_sem=rs_recv.at[j % 3, pair + kind, s], device_id=peer(*to), device_id_type=MESH,
        ).start()

    def rep_copy(j, send, recv):
        return pltpu.make_async_remote_copy(
            src_ref=g.at[j, own["z"], own["y"], own["x"]], dst_ref=rep_in.at[j], send_sem=send, recv_sem=recv,
            device_id=peer("z", 2), device_id_type=MESH,
        )

    def rep_sems(j):
        return rs_send.at[0, 5], rs_recv.at[j % 3, 0, 5]

    def rs_collect(j, s, pair, kind=0):
        await_stage(RS_SHARDS[s - 1][0 if kind else pair], rs_send.at[pair + kind, s - 1], rs_recv.at[j % 3, pair + kind, s - 1])
        for plan in rs_plans[kind][2 * pair : 2 * pair + 2]:
            for _, _, _, at, slot, target in plan[s - 1]:
                to = region(j, *target)
                g[to] = (g[to].astype(F32) + land(kind, j, at, slot)[...].astype(F32)).astype(BF16)

    def rs_stage(j, s):
        for pair in (1, 0) if s in (2, 4) else (0, 1):
            def part(kind):
                if s >= 1:
                    rs_collect(j, s, pair, kind)
                if s < 5:
                    for plan in rs_plans[kind][2 * pair : 2 * pair + 2]:
                        for t in plan[s]:
                            rs_start(j, s, pair, kind, t)

            per_kind(j, pair, part)
        if s == 5:
            rep_copy(j, *rep_sems(j)).start()

    def rs_last_ring(j):
        for pair in (0, 1):
            rs_collect(j, 3, pair)
            for q in (2 * pair, 2 * pair + 1):
                axis = ORDERS[q][0]
                for k, by in enumerate((2, 1, -1)):
                    pltpu.make_async_remote_copy(
                        src_ref=g.at[region(j, q, sel_of((), axis, shifted(axis, by)), 2)], dst_ref=last_in.at[q, k],
                        send_sem=once.at[2], recv_sem=once.at[3], device_id=peer(axis, by), device_id_type=MESH,
                    ).start()

    def rs_last_sum(j):
        await_stage(3, once.at[2], once.at[3])
        for q, order in enumerate(ORDERS):
            to = region(j, q, sel_of((), order[0], own[order[0]]), 2)
            g[to] = (g[to].astype(F32) + last_in[q, 0].astype(F32) + last_in[q, 1].astype(F32) + last_in[q, 2].astype(F32)).astype(BF16)
        rep_copy(j, once.at[4], once.at[5]).start()

    def choose(usual, for_last):
        def stage(j):
            if usual is not None:
                @pl.when(j < blocks - 1)
                def _():
                    usual(j)

            if for_last is not None:
                @pl.when(j == blocks - 1)
                def _():
                    for_last(j)

        return stage

    def rs_finish(j, sems=rep_sems):
        rep_copy(j, *sems(j)).wait()
        total = g[j, own["z"], own["y"], own["x"]].astype(F32) + rep_in[j].astype(F32)
        columns = pl.ds(pl.multiple_of(j * HALF, HALF), HALF)
        run[0, :, columns] = run[0, :, columns] + factor * total[:, :HALF]
        run[1, :, columns] = run[1, :, columns] + factor * total[:, HALF:]
        pltpu.make_async_copy(run.at[0, :, columns], gtot_hbm.at[:, columns], out_sem.at[2]).start()
        pltpu.make_async_copy(run.at[1, :, columns], utot_hbm.at[:, columns], out_sem.at[2]).start()

    def tp_copy(i, ref):
        return pltpu.make_async_remote_copy(
            src_ref=ref, dst_ref=ref, send_sem=tp_send.at[i], recv_sem=tp_recv.at[i], device_id={"tp": 1 - tp}, device_id_type=MESH
        )

    def tp_received(i, ref):
        return pltpu.make_async_remote_copy(
            src_ref=ref, dst_ref=ref, send_sem=tp_send.at[i], recv_sem=tp_recv.at[i], device_id={"tp": 1 - tp}, device_id_type=MESH
        )

    def dn_copy():
        return pltpu.make_async_remote_copy(
            src_ref=dn.at[1], dst_ref=dn.at[2], send_sem=tp_send.at[3], recv_sem=tp_recv.at[3], device_id={"tp": 1 - tp}, device_id_type=MESH
        )

    loads = [
        pltpu.make_async_copy(later_hbm, xin.at[0], load_sem.at[0]),
        pltpu.make_async_copy(earlier_hbm, xin.at[1], load_sem.at[1]),
        pltpu.make_async_copy(cot_hbm, cot, load_sem.at[2]),
        pltpu.make_async_copy(grun_hbm, run.at[0], load_sem.at[3]),
        pltpu.make_async_copy(urun_hbm, run.at[1], load_sem.at[4]),
    ]

    def shard_loads(j):
        columns = pl.ds(pl.multiple_of(j * HALF, HALF), HALF)
        mine = (j, own["z"], own["y"], own["x"], ALL)
        return [
            pltpu.make_async_copy(gw_hbm.at[:, columns], w.at[(*mine, pl.ds(0, HALF))], w_sem.at[0]),
            pltpu.make_async_copy(uw_hbm.at[:, columns], w.at[(*mine, pl.ds(HALF, HALF))], w_sem.at[0]),
        ]

    @pl.loop(0, blocks)
    def _(j):
        for c in shard_loads(j):
            c.start()

    for c in loads:
        c.start()

    barrier = pltpu.get_barrier_semaphore()
    greeted = [peer(a, by) for a in "xyz" for by in (1, 2, 3)] + [{"tp": 1 - tp}]
    for device in greeted:
        pl.semaphore_signal(barrier, inc=1, device_id=device, device_id_type=MESH)
    pl.semaphore_wait(barrier, len(greeted))

    pltpu.make_async_copy(w.at[:, own["z"], own["y"], own["x"]], w.at[:, own["z"], own["y"], own["x"]], w_sem.at[0]).wait()
    ag_first()
    ag_early(0, 0)
    ag_early(0, 1)

    step_rows = 32 if rows % 32 == 0 else rows

    def normalize(m, out):
        @pl.loop(0, rows // step_rows)
        def _(i):
            at = pl.ds(pl.multiple_of(i * step_rows, step_rows), step_rows)
            values = xin[m, at, :].astype(F32)
            inv = lax.rsqrt(jnp.mean(values * values, axis=1, keepdims=True) + EPSILON)
            out[tp, at, :] = (values * inv * gain_ref[...]).astype(BF16)
            if m == 1:
                inv_ref[at, :] = inv

    def prepare(t):
        if t == 0:
            for c in loads:
                c.wait()
            normalize(1, xe)
            tp_copy(1, xe.at[tp]).start()
        elif t == 1:
            slab, mine = min(256, width), pl.ds(pl.multiple_of(tp * rows, rows), rows)

            @pl.loop(0, width // slab)
            def _(i):
                at = pl.ds(pl.multiple_of(i * slab, slab), slab)
                xt[at, mine] = xe[tp, :, at].T

            tp_copy(2, xt.at[:, mine]).start()
        elif t == 2:
            normalize(0, xl)
            tp_copy(0, xl.at[tp]).start()
        elif t == 3:
            acc[...] = jnp.zeros_like(acc)
        else:
            exchanged()

    def exchanged():
        for i, ref in ((0, xl), (1, xe)):
            tp_copy(i, ref.at[tp]).wait_send()
            tp_received(i, ref.at[1 - tp]).wait_recv()
        tp_copy(2, xt.at[:, pl.ds(pl.multiple_of(tp * rows, rows), rows)]).wait_send()
        tp_received(2, xt.at[:, pl.ds(pl.multiple_of((1 - tp) * rows, rows), rows)]).wait_recv()

    def block_weight(j):
        return w[j].reshape(width, 2 * HALF)

    def backward(j):
        columns = pl.ds(pl.multiple_of(j * HALF, HALF), HALF)

        @pl.loop(0, 2)
        def _(m):
            both = jnp.dot(xe[m], block_weight(j), preferred_element_type=F32)
            gate, up = both[:, :HALF], both[:, HALF:]
            s = sigmoid(gate)
            c = cot[pl.ds(pl.multiple_of(m * rows, rows), rows), columns].astype(F32)
            d[m, :, 0:HALF] = (c * up * s * (1.0 + gate * (1.0 - s))).astype(BF16)
            d[m, :, HALF:] = (c * gate * s).astype(BF16)

        @pl.loop(0, 4)
        def _(k):
            z, y = k // 2, 2 * (k % 2)
            at = pl.ds(pl.multiple_of(k * (width // 4), width // 4), width // 4)
            part = jnp.dot(xt[at, :], d[...].reshape(2 * rows, 2 * HALF), preferred_element_type=F32)
            g[j, z, pl.ds(y, 2)] = part.astype(BF16).reshape(2, 4, 4 * quarter, 2 * HALF)

    def later(j):
        @pl.loop(0, 2)
        def _(m):
            both = jnp.dot(xl[m], block_weight(j), preferred_element_type=F32)
            gate, up = both[:, :HALF], both[:, HALF:]
            lh[j, pl.ds(pl.multiple_of(m * rows, rows), rows), :] = (gate * sigmoid(gate) * up).astype(BF16)

        hidden_copy(j).start()

    def hidden_copy(j):
        columns = pl.ds(pl.multiple_of(j * HALF, HALF), HALF)
        return pltpu.make_async_copy(lh.at[j], hidden_hbm.at[:, columns], out_sem.at[0])

    def input_gradient(j):
        @pl.loop(0, 4)
        def _(k):
            z, y = k // 2, 2 * (k % 2)
            at = pl.ds(pl.multiple_of(k * (width // 4), width // 4), width // 4)
            part = w[j, z, pl.ds(y, 2)].reshape(width // 4, 2 * HALF)
            for m in range(2):
                acc[m, :, at] = acc[m, :, at] + lax.dot_general(
                    d[m], part, (((1,), (1,)), ((), ())), preferred_element_type=F32
                )

    def send_input_gradient():
        @pl.loop(0, rows // step_rows)
        def _(i):
            at = pl.ds(pl.multiple_of(i * step_rows, step_rows), step_rows)
            dn[0, at, :] = acc[tp, at, :].astype(BF16)
            dn[1, at, :] = acc[1 - tp, at, :].astype(BF16)

        dn_copy().start()

    def finish_input_gradient():
        dn_copy().wait()
        gain = gain_ref[...]
        own_slot = gbuf.at[0, own["x"]]
        own_slot[...] = jnp.zeros_like(own_slot)

        @pl.loop(0, rows // step_rows)
        def _(i):
            at = pl.ds(pl.multiple_of(i * step_rows, step_rows), step_rows)
            d_norm = dn[0, at, :].astype(F32) + dn[2, at, :].astype(F32)
            values = xin[1, at, :].astype(F32)
            inv = inv_ref[at, :]
            scaled = d_norm * gain
            inner = jnp.mean(scaled * values, axis=1, keepdims=True)
            dn[1, at, :] = (inv * scaled - values * (inv * inv * inv) * inner).astype(BF16)
            own_slot[...] = own_slot[...] + jnp.sum(d_norm * values * inv, axis=0, keepdims=True)

        grad_copy().start()

    def grad_copy():
        return pltpu.make_async_copy(dn.at[1], grad_hbm, out_sem.at[1])

    def gain_copies(r):
        axis = ("x", "y", "z")[r]
        at = (own["x"], own["y"], ring_z)[r]
        return [
            pltpu.make_async_remote_copy(
                src_ref=gbuf.at[r, at], dst_ref=gbuf.at[r, at], send_sem=gain_send.at[3 * r + k - 1], recv_sem=gain_recv.at[3 * r + k - 1],
                device_id=peer(axis, k), device_id_type=MESH,
            )
            for k in (1, 2, 3)
        ]

    def gain_received(r):
        axis = ("x", "y", "z")[r]
        at = (own["x"], own["y"], ring_z)[r]
        return [
            pltpu.make_async_remote_copy(
                src_ref=gbuf.at[r, at], dst_ref=gbuf.at[r, (at - k) % 4], send_sem=gain_send.at[3 * r + k - 1], recv_sem=gain_recv.at[3 * r + k - 1],
                device_id=peer(axis, k), device_id_type=MESH,
            )
            for k in (1, 2, 3)
        ]

    def gain_sum(r):
        for c in gain_received(r):
            c.wait()
        return (gbuf[r, 0] + gbuf[r, 1]) + (gbuf[r, 2] + gbuf[r, 3])

    def gain_tp():
        return pltpu.make_async_remote_copy(
            src_ref=gbuf.at[3, 0], dst_ref=gbuf.at[3, 1], send_sem=gain_send.at[9], recv_sem=gain_recv.at[9],
            device_id={"tp": 1 - tp}, device_id_type=MESH,
        )

    def gain_step(r):
        if r == 0:
            finish_input_gradient()
            for c in gain_copies(0):
                c.start()
        elif r < 3:
            gbuf[r, (own["x"], own["y"], ring_z)[r]] = gain_sum(r - 1)
            for c in gain_copies(r):
                c.start()
        elif r == 3:
            gbuf[3, 0] = gain_sum(2)
            gain_tp().start()
        else:
            gain_tp().wait()
            gain_tot[...] = gain_run[...] + factor * (gbuf[3, 0] + gbuf[3, 1])

    last = 4 + blocks - 1

    @pl.loop(0, last + 6)
    def _(t):
        def at_stage(offset, run_stage):
            j = t - offset

            @pl.when((j >= 0) & (j < blocks))
            def _():
                run_stage(j)

        for s in (5, 4, 3):
            at_stage(s - 1, functools.partial(ag_stage, s=s))
        at_stage(1, ag_second)

        for k in (0, 1):
            @pl.when(t == 1 + k)
            def _():
                ag_early(1, k)
        for k in range(5):
            @pl.when(t == k)
            def _():
                prepare(k)

        at_stage(4, backward)
        at_stage(10, choose(rs_finish, None))
        at_stage(9, choose(functools.partial(rs_stage, s=5), lambda j: rs_finish(j, lambda _: (once.at[4], once.at[5]))))
        at_stage(8, choose(functools.partial(rs_stage, s=4), rs_last_sum))
        at_stage(7, choose(functools.partial(rs_stage, s=3), rs_last_ring))
        at_stage(6, functools.partial(rs_stage, s=2))
        at_stage(5, functools.partial(rs_stage, s=1))
        at_stage(4, functools.partial(rs_stage, s=0))
        at_stage(4, later)
        at_stage(4, input_gradient)

        @pl.when(t == last)
        def _():
            send_input_gradient()

        for r in range(5):
            @pl.when(t == last + 1 + r)
            def _():
                gain_step(r)

    pltpu.make_async_copy(lh, lh, out_sem.at[0]).wait()
    grad_copy().wait()
    pltpu.make_async_copy(run, run, out_sem.at[2]).wait()


def copy_kernel(*refs):
    n = (len(refs) - 2) // 3
    sources, results, held, (into, back) = refs[:n], refs[n : 2 * n], refs[2 * n : 3 * n], refs[3 * n :]
    reads = [pltpu.make_async_copy(a, b, into.at[i]) for i, (a, b) in enumerate(zip(sources, held))]
    writes = [pltpu.make_async_copy(a, b, back.at[i]) for i, (a, b) in enumerate(zip(held, results))]
    for c in reads:
        c.start()
    for a, b in zip(reads, writes):
        a.wait()
        b.start()
    for c in writes:
        c.wait()


def copied(*arrays):
    n = len(arrays)
    hbm = pl.BlockSpec(memory_space=pl.ANY)
    return pl.pallas_call(
        copy_kernel,
        out_shape=tuple(jax.ShapeDtypeStruct(a.shape, a.dtype) for a in arrays),
        in_specs=[hbm] * n,
        out_specs=(hbm,) * n,
        scratch_shapes=[*[pltpu.VMEM(a.shape, a.dtype) for a in arrays], pltpu.SemaphoreType.DMA((n,)), pltpu.SemaphoreType.DMA((n,))],
        compiler_params=pltpu.CompilerParams(vmem_limit_bytes=67043328),
        name="hand_over",
    )(*arrays)


def body(later_input, earlier_input, hidden_cot, norm_gain, gate_weight, up_weight, gate_running, up_running, gain_running):
    rows, width = later_input.shape
    shard, hidden = gate_weight.shape
    blocks = hidden // HALF
    quarter = shard // 4
    tokens = rows * lax.axis_size("rep") * lax.axis_size("fs") * lax.axis_size("tp")
    factor = 1.0 / math.sqrt(tokens)
    whole = (blocks, 2, 4, 4, shard, 2 * HALF)
    hbm = pl.BlockSpec(memory_space=pl.ANY)
    vmem = pl.BlockSpec(memory_space=pltpu.VMEM)
    dma = pltpu.SemaphoreType.DMA
    out = pl.pallas_call(
        functools.partial(kernel, blocks, factor),
        out_shape=(
            jax.ShapeDtypeStruct((2 * rows, hidden), BF16),
            jax.ShapeDtypeStruct((rows, width), BF16),
            jax.ShapeDtypeStruct((shard, hidden), F32),
            jax.ShapeDtypeStruct((shard, hidden), F32),
            jax.ShapeDtypeStruct((1, width), F32),
        ),
        in_specs=[hbm, hbm, hbm, vmem, hbm, hbm, hbm, hbm, vmem],
        out_specs=(hbm, hbm, hbm, hbm, vmem),
        scratch_shapes=[
            pltpu.VMEM(whole, BF16),
            pltpu.VMEM(whole, BF16),
            pltpu.VMEM((2, rows, width), BF16),
            pltpu.VMEM((2, rows, width), BF16),
            pltpu.VMEM((2, rows, width), BF16),
            pltpu.VMEM((width, 2 * rows), BF16),
            pltpu.VMEM((2 * rows, hidden), BF16),
            pltpu.VMEM((2, rows, 2 * HALF), BF16),
            pltpu.VMEM((2, rows, width), F32),
            pltpu.VMEM((blocks, 2 * rows, HALF), BF16),
            pltpu.VMEM((3, rows, width), BF16),
            pltpu.VMEM((rows, 1), F32),
            pltpu.VMEM((2, shard, hidden), F32),
            pltpu.VMEM((4, 4, 1, width), F32),
            pltpu.VMEM((blocks, shard, 2 * HALF), BF16),
            pltpu.VMEM((4, 3, quarter, 2 * HALF), BF16),
            *[pltpu.VMEM(s, BF16) for s in landing_shapes(ORDERS, blocks, quarter)],
            *[pltpu.VMEM(s, BF16) for s in landing_shapes(ORDERS_MID, 1, quarter)],
            dma((3, 3)),
            dma((3, 3, 3)),
            dma((2, 2, 2)),
            dma((3, 6)),
            dma((3, 3, 6)),
            dma((6,)),
            dma((5,)),
            dma((1,)),
            dma((4,)),
            dma((4,)),
            dma((2, 10)),
            dma((3,)),
        ],
        compiler_params=pltpu.CompilerParams(collective_id=0, has_side_effects=True, vmem_limit_bytes=67043328),
        cost_estimate=pl.CostEstimate(flops=16 * rows * width * hidden * 2, bytes_accessed=16 << 20, transcendentals=0),
        name="half_step",
    )(
        later_input, earlier_input, hidden_cot, norm_gain.reshape(1, width), gate_weight, up_weight, gate_running, up_running,
        gain_running.reshape(1, width),
    )
    hidden_out, grad, gate_total, up_total, gain_total = copied(*out)
    return hidden_out, grad, gate_total, up_total, gain_total.reshape(width)


def solution(mesh):
    in_specs = (
        P(("rep", "fs", "tp"), None),
        P(("rep", "fs", "tp"), None),
        P(("rep", "fs"), "tp"),
        P(),
        P("fs", "tp"),
        P("fs", "tp"),
        P("fs", "tp"),
        P("fs", "tp"),
        P(),
    )
    out_specs = (
        P(("rep", "fs"), "tp"),
        P(("rep", "fs", "tp"), None),
        P("fs", "tp"),
        P("fs", "tp"),
        P(),
    )
    return jax.shard_map(body, mesh=mesh, in_specs=in_specs, out_specs=out_specs, check_vma=False)
```

```python
import functools
import math

import jax
import jax.numpy as jnp
from jax import lax
from jax.experimental import pallas as pl
from jax.experimental.pallas import tpu as pltpu
from jax.sharding import PartitionSpec as P

EPSILON = 1e-06
MESH = pl.DeviceIdType.MESH
HALF = 128
F32, BF16 = jnp.float32, jnp.bfloat16
SIZE = {"z": 2, "y": 4, "x": 4}
ORDERS = (("y", "z", "x"), ("x", "z", "y"), ("x", "y", "z"), ("y", "x", "z"))
ORDERS_MID = ORDERS[:2] + (("x", "z", "y"), ("y", "z", "x"))
ALL = slice(None)
AG_SHARDS = ((1, 1), (0.5, 0.5), (2, 4), (8, 2), (4, 8))
RS_SHARDS = ((4, 8), (8, 2), (2, 4), (0.5, 0.5), (1, 1))


def sigmoid(v):
    return 1.0 / (1.0 + jnp.exp(-v))


def landing_shapes(orders, blocks, quarter):
    shapes = []
    for order in orders:
        full = [a for a in "zyx"]
        for axis in reversed(order):
            full.remove(axis)
            lead = tuple(SIZE[a] for a in full)
            if axis == "z":
                shapes.append((blocks, 2, *lead, quarter, HALF))
            else:
                shapes.append((blocks, 2, *lead, quarter, HALF))
                shapes.append((blocks, 2, *lead, quarter, 2 * HALF))
    return shapes


def kernel(
    blocks, factor, later_hbm, earlier_hbm, cot_hbm, gain_ref, gw_hbm, uw_hbm, grun_hbm, urun_hbm, gain_run,
    hidden_out, grad_out, gtot_out, utot_out, gain_tot,
    w, g, xin, xl, xe, xt, cot, d, acc, dn, inv_ref, run, gbuf, rep_in, *rest,
):
    last_in, landing = rest[0], list(rest[1:-11])
    ag_send, ag_recv, early, rs_send, rs_recv, once, load_sem, w_sem, tp_send, tp_recv, gs = rest[-11:]
    gain_send, gain_recv = gs.at[0], gs.at[1]
    rows = xin.shape[1]
    width = xin.shape[2]
    quarter = g.shape[4] // 4
    rep, fs, tp = lax.axis_index("rep"), lax.axis_index("fs"), lax.axis_index("tp")
    own = {"x": fs % 4, "y": (fs // 4) % 4, "z": fs // 16}
    ring_z = 2 * rep + own["z"]

    def peer(axis, by):
        if axis == "z":
            z = (ring_z + by) % 4
            return {"rep": z // 2, "fs": (z % 2) * 16 + own["y"] * 4 + own["x"]}
        c = (own[axis] + by) % 4
        if axis == "y":
            return {"fs": own["z"] * 16 + c * 4 + own["x"]}
        return {"fs": own["z"] * 16 + own["y"] * 4 + c}

    def shifted(axis, by):
        return (1 - own["z"] if by else own["z"]) if axis == "z" else (own[axis] + by) % 4

    HALVES = (pl.ds(0, HALF), pl.ds(HALF, HALF), pl.ds(0, 2 * HALF))

    def region(j, q, sel, half):
        return (j, sel["z"], sel["y"], sel["x"], pl.ds(q * quarter, quarter), HALVES[half])

    def sel_of(full, axis, coordinate):
        s = {a: (ALL if a in full else own[a]) for a in "zyx"}
        s[axis] = coordinate
        return s

    def plan_gather(orders):
        plans, count = [], 0
        for q, order in enumerate(orders):
            phases = []
            for p, axis in enumerate(order):
                full = order[:p]
                if axis == "z":
                    group = []
                    for k, by in enumerate((1, -1)):
                        group.append((count, (q, sel_of(full, "z", own["z"]), k), ("z", by), (q, sel_of(full, "z", 1 - own["z"]), k)))
                        count += 1
                    phases.append(("z", [group]))
                else:
                    first, second = [], []
                    for k, by in enumerate((1, -1)):
                        first.append((count, (q, sel_of(full, axis, own[axis]), 2), (axis, by), (q, sel_of(full, axis, shifted(axis, -by)), 2)))
                        count += 1
                    for k, by in enumerate((1, -1)):
                        second.append((count, (q, sel_of(full, axis, shifted(axis, -by)), k), (axis, by), (q, sel_of(full, axis, shifted(axis, 2)), k)))
                        count += 1
                    phases.append((axis, [first, second]))
            plans.append([group for _, groups in phases for group in groups])
        return plans

    ag_plans = plan_gather(ORDERS), plan_gather(ORDERS_MID)
    ag_plan = ag_plans[0]

    def shards(n):
        if n <= 4:
            if n == 0.5:
                return w.at[0, 0, 0, 0, pl.ds(0, 2 * quarter)]
            return w.at[0, 0, 0, pl.ds(0, n)]
        if n % 4 == 0:
            return w.at[0, 0, pl.ds(0, n // 4)]
        return w.at[:, 0, 0, 0]

    def await_stage(n, send, recv):
        pltpu.make_async_copy(shards(n), shards(n), send).wait()
        pltpu.make_async_copy(shards(n), shards(n), recv).wait()

    def ag_send_to(j, src, to, send, recv):
        pltpu.make_async_remote_copy(
            src_ref=w.at[region(j, *src)], dst_ref=w.at[region(j, *src)], send_sem=send, recv_sem=recv, device_id=peer(*to), device_id_type=MESH
        ).start()

    middle = blocks // 2

    def per_kind(j, pair, run):
        if pair == 0:
            run(0)
            return

        @pl.when(j != middle)
        def _():
            run(0)

        @pl.when(j == middle)
        def _():
            run(1)

    def ag_stage(j, s, wait=True):
        for pair in (1, 0):
            def part(kind):
                if wait:
                    await_stage(AG_SHARDS[s - 1][0 if kind else pair], ag_send.at[pair + kind, s - 3], ag_recv.at[j % 3, pair + kind, s - 3])
                if s < 5:
                    for plan in ag_plans[kind][2 * pair : 2 * pair + 2]:
                        for _, src, to, _ in plan[s]:
                            ag_send_to(j, src, to, ag_send.at[pair + kind, s - 2], ag_recv.at[j % 3, pair + kind, s - 2])

            per_kind(j, pair, part)

    def ag_first():
        for q, order in enumerate(ORDERS):
            src = (q, sel_of((), order[0], own[order[0]]), 2)
            for by in (2, 1, -1):
                ag_send_to(0, src, (order[0], by), once.at[0], once.at[1])

    groups = (pl.ds(1, 1), pl.ds(2, blocks - 2))

    def ag_early(s, k):
        if s == 1:
            await_early(0, k)
        for plan in ag_plan:
            for _, src, to, _ in plan[s]:
                ag_send_to(groups[k], src, to, early.at[k, 0, s], early.at[k, 1, s])

    def await_early(s, k):
        for way in (0, 1):
            view = w.at[groups[k], 0, 0, pl.ds(0, 2)] if s == 0 else w.at[groups[k], 0, 0, 0]
            pltpu.make_async_copy(view, view, early.at[k, way, s]).wait()

    def ag_second(j):
        @pl.when(j == 0)
        def _():
            await_stage(3, once.at[0], once.at[1])

        for k in (0, 1):
            @pl.when(j == 1 + k)
            def _():
                await_early(1, k)

        ag_stage(j, 2, wait=False)

    def plan_scatter(orders, place):
        plans, count = [], 0
        for q, order in enumerate(orders):
            groups = []
            full = ["z", "y", "x"]
            for axis in reversed(order):
                full.remove(axis)
                if axis == "z":
                    group = []
                    for k, by in enumerate((1, -1)):
                        group.append((count, (q, sel_of(full, "z", 1 - own["z"]), k), ("z", by), place, k, (q, sel_of(full, "z", own["z"]), k)))
                        count += 1
                    groups.append(group)
                    place += 1
                else:
                    first, second = [], []
                    for k, by in enumerate((1, -1)):
                        first.append((count, (q, sel_of(full, axis, shifted(axis, 2)), k), (axis, by), place, k, (q, sel_of(full, axis, shifted(axis, by)), k)))
                        count += 1
                    for k, by in enumerate((1, -1)):
                        second.append((count, (q, sel_of(full, axis, shifted(axis, by)), 2), (axis, by), place + 1, k, (q, sel_of(full, axis, own[axis]), 2)))
                        count += 1
                    groups += [first, second]
                    place += 2
            plans.append(groups)
        return plans

    half_landing = len(landing) // 2
    rs_plans = plan_scatter(ORDERS, 0), plan_scatter(ORDERS_MID, half_landing)

    def land(kind, j, at, slot):
        return landing[at].at[0 if kind else j, slot]

    def rs_start(j, s, pair, kind, t):
        _, src, to, at, slot, _ = t
        pltpu.make_async_remote_copy(
            src_ref=g.at[region(j, *src)], dst_ref=land(kind, j, at, slot), send_sem=rs_send.at[pair + kind, s],
            recv_sem=rs_recv.at[j % 3, pair + kind, s], device_id=peer(*to), device_id_type=MESH,
        ).start()

    def rep_copy(j, send, recv):
        return pltpu.make_async_remote_copy(
            src_ref=g.at[j, own["z"], own["y"], own["x"]], dst_ref=rep_in.at[j], send_sem=send, recv_sem=recv,
            device_id=peer("z", 2), device_id_type=MESH,
        )

    def rep_sems(j):
        return rs_send.at[0, 5], rs_recv.at[j % 3, 0, 5]

    def rs_collect(j, s, pair, kind=0):
        await_stage(RS_SHARDS[s - 1][0 if kind else pair], rs_send.at[pair + kind, s - 1], rs_recv.at[j % 3, pair + kind, s - 1])
        for plan in rs_plans[kind][2 * pair : 2 * pair + 2]:
            for _, _, _, at, slot, target in plan[s - 1]:
                to = region(j, *target)
                g[to] = (g[to].astype(F32) + land(kind, j, at, slot)[...].astype(F32)).astype(BF16)

    def rs_stage(j, s):
        for pair in (1, 0) if s in (2, 4) else (0, 1):
            def part(kind):
                if s >= 1:
                    rs_collect(j, s, pair, kind)
                if s < 5:
                    for plan in rs_plans[kind][2 * pair : 2 * pair + 2]:
                        for t in plan[s]:
                            rs_start(j, s, pair, kind, t)

            per_kind(j, pair, part)
        if s == 5:
            rep_copy(j, *rep_sems(j)).start()

    def rs_last_ring(j):
        for pair in (0, 1):
            rs_collect(j, 3, pair)
            for q in (2 * pair, 2 * pair + 1):
                axis = ORDERS[q][0]
                for k, by in enumerate((2, 1, -1)):
                    pltpu.make_async_remote_copy(
                        src_ref=g.at[region(j, q, sel_of((), axis, shifted(axis, by)), 2)], dst_ref=last_in.at[q, k],
                        send_sem=once.at[2], recv_sem=once.at[3], device_id=peer(axis, by), device_id_type=MESH,
                    ).start()

    def rs_last_sum(j):
        await_stage(3, once.at[2], once.at[3])
        for q, order in enumerate(ORDERS):
            to = region(j, q, sel_of((), order[0], own[order[0]]), 2)
            g[to] = (g[to].astype(F32) + last_in[q, 0].astype(F32) + last_in[q, 1].astype(F32) + last_in[q, 2].astype(F32)).astype(BF16)
        rep_copy(j, once.at[4], once.at[5]).start()

    def choose(usual, for_last):
        def stage(j):
            if usual is not None:
                @pl.when(j < blocks - 1)
                def _():
                    usual(j)

            if for_last is not None:
                @pl.when(j == blocks - 1)
                def _():
                    for_last(j)

        return stage

    def rs_finish(j, sems=rep_sems):
        rep_copy(j, *sems(j)).wait()
        total = g[j, own["z"], own["y"], own["x"]].astype(F32) + rep_in[j].astype(F32)
        columns = pl.ds(pl.multiple_of(j * HALF, HALF), HALF)
        gtot_out[:, columns] = run[0, :, columns] + factor * total[:, :HALF]
        utot_out[:, columns] = run[1, :, columns] + factor * total[:, HALF:]

    def tp_copy(i, ref):
        return pltpu.make_async_remote_copy(
            src_ref=ref, dst_ref=ref, send_sem=tp_send.at[i], recv_sem=tp_recv.at[i], device_id={"tp": 1 - tp}, device_id_type=MESH
        )

    def tp_received(i, ref):
        return pltpu.make_async_remote_copy(
            src_ref=ref, dst_ref=ref, send_sem=tp_send.at[i], recv_sem=tp_recv.at[i], device_id={"tp": 1 - tp}, device_id_type=MESH
        )

    def dn_copy():
        return pltpu.make_async_remote_copy(
            src_ref=dn.at[1], dst_ref=dn.at[2], send_sem=tp_send.at[3], recv_sem=tp_recv.at[3], device_id={"tp": 1 - tp}, device_id_type=MESH
        )

    loads = [
        pltpu.make_async_copy(later_hbm, xin.at[0], load_sem.at[0]),
        pltpu.make_async_copy(earlier_hbm, xin.at[1], load_sem.at[1]),
        pltpu.make_async_copy(cot_hbm, cot, load_sem.at[2]),
        pltpu.make_async_copy(grun_hbm, run.at[0], load_sem.at[3]),
        pltpu.make_async_copy(urun_hbm, run.at[1], load_sem.at[4]),
    ]

    def shard_loads(j):
        columns = pl.ds(pl.multiple_of(j * HALF, HALF), HALF)
        mine = (j, own["z"], own["y"], own["x"], ALL)
        return [
            pltpu.make_async_copy(gw_hbm.at[:, columns], w.at[(*mine, pl.ds(0, HALF))], w_sem.at[0]),
            pltpu.make_async_copy(uw_hbm.at[:, columns], w.at[(*mine, pl.ds(HALF, HALF))], w_sem.at[0]),
        ]

    @pl.loop(0, blocks)
    def _(j):
        for c in shard_loads(j):
            c.start()

    for c in loads:
        c.start()

    barrier = pltpu.get_barrier_semaphore()
    greeted = [peer(a, by) for a in "xyz" for by in (1, 2, 3)] + [{"tp": 1 - tp}]
    for device in greeted:
        pl.semaphore_signal(barrier, inc=1, device_id=device, device_id_type=MESH)
    pl.semaphore_wait(barrier, len(greeted))

    pltpu.make_async_copy(w.at[:, own["z"], own["y"], own["x"]], w.at[:, own["z"], own["y"], own["x"]], w_sem.at[0]).wait()
    ag_first()
    ag_early(0, 0)
    ag_early(0, 1)

    step_rows = 32 if rows % 32 == 0 else rows

    def normalize(m, out):
        @pl.loop(0, rows // step_rows)
        def _(i):
            at = pl.ds(pl.multiple_of(i * step_rows, step_rows), step_rows)
            values = xin[m, at, :].astype(F32)
            inv = lax.rsqrt(jnp.mean(values * values, axis=1, keepdims=True) + EPSILON)
            out[tp, at, :] = (values * inv * gain_ref[...]).astype(BF16)
            if m == 1:
                inv_ref[at, :] = inv

    def prepare(t):
        if t == 0:
            for c in loads:
                c.wait()
            normalize(1, xe)
            tp_copy(1, xe.at[tp]).start()
        elif t == 1:
            slab, mine = min(256, width), pl.ds(pl.multiple_of(tp * rows, rows), rows)

            @pl.loop(0, width // slab)
            def _(i):
                at = pl.ds(pl.multiple_of(i * slab, slab), slab)
                xt[at, mine] = xe[tp, :, at].T

            tp_copy(2, xt.at[:, mine]).start()
        elif t == 2:
            normalize(0, xl)
            tp_copy(0, xl.at[tp]).start()
        elif t == 3:
            acc[...] = jnp.zeros_like(acc)
        else:
            exchanged()

    def exchanged():
        for i, ref in ((0, xl), (1, xe)):
            tp_copy(i, ref.at[tp]).wait_send()
            tp_received(i, ref.at[1 - tp]).wait_recv()
        tp_copy(2, xt.at[:, pl.ds(pl.multiple_of(tp * rows, rows), rows)]).wait_send()
        tp_received(2, xt.at[:, pl.ds(pl.multiple_of((1 - tp) * rows, rows), rows)]).wait_recv()

    def block_weight(j):
        return w[j].reshape(width, 2 * HALF)

    def backward(j):
        columns = pl.ds(pl.multiple_of(j * HALF, HALF), HALF)

        for m in range(2):
            both = jnp.dot(xe[m], block_weight(j), preferred_element_type=F32)
            gate, up = both[:, :HALF], both[:, HALF:]
            s = sigmoid(gate)
            c = cot[pl.ds(m * rows, rows), columns].astype(F32)
            d[m, :, 0:HALF] = (c * up * s * (1.0 + gate * (1.0 - s))).astype(BF16)
            d[m, :, HALF:] = (c * gate * s).astype(BF16)

        for k in range(4):
            z, y = k // 2, 2 * (k % 2)
            at = pl.ds(k * (width // 4), width // 4)
            part = jnp.dot(xt[at, :], d[...].reshape(2 * rows, 2 * HALF), preferred_element_type=F32)
            g[j, z, pl.ds(y, 2)] = part.astype(BF16).reshape(2, 4, 4 * quarter, 2 * HALF)

    def later(j):
        columns = pl.ds(pl.multiple_of(j * HALF, HALF), HALF)

        @pl.loop(0, 2)
        def _(m):
            both = jnp.dot(xl[m], block_weight(j), preferred_element_type=F32)
            gate, up = both[:, :HALF], both[:, HALF:]
            hidden_out[pl.ds(pl.multiple_of(m * rows, rows), rows), columns] = (gate * sigmoid(gate) * up).astype(BF16)

    def input_gradient(j):
        @pl.loop(0, 4)
        def _(k):
            z, y = k // 2, 2 * (k % 2)
            at = pl.ds(pl.multiple_of(k * (width // 4), width // 4), width // 4)
            part = w[j, z, pl.ds(y, 2)].reshape(width // 4, 2 * HALF)
            for m in range(2):
                acc[m, :, at] = acc[m, :, at] + lax.dot_general(
                    d[m], part, (((1,), (1,)), ((), ())), preferred_element_type=F32
                )

    def send_input_gradient():
        @pl.loop(0, rows // step_rows)
        def _(i):
            at = pl.ds(pl.multiple_of(i * step_rows, step_rows), step_rows)
            dn[0, at, :] = acc[tp, at, :].astype(BF16)
            dn[1, at, :] = acc[1 - tp, at, :].astype(BF16)

        dn_copy().start()

    def finish_input_gradient():
        dn_copy().wait()
        gain = gain_ref[...]
        own_slot = gbuf.at[0, own["x"]]
        own_slot[...] = jnp.zeros_like(own_slot)

        @pl.loop(0, rows // step_rows)
        def _(i):
            at = pl.ds(pl.multiple_of(i * step_rows, step_rows), step_rows)
            d_norm = dn[0, at, :].astype(F32) + dn[2, at, :].astype(F32)
            values = xin[1, at, :].astype(F32)
            inv = inv_ref[at, :]
            scaled = d_norm * gain
            inner = jnp.mean(scaled * values, axis=1, keepdims=True)
            grad_out[at, :] = (inv * scaled - values * (inv * inv * inv) * inner).astype(BF16)
            own_slot[...] = own_slot[...] + jnp.sum(d_norm * values * inv, axis=0, keepdims=True)

    def gain_copies(r):
        axis = ("x", "y", "z")[r]
        at = (own["x"], own["y"], ring_z)[r]
        return [
            pltpu.make_async_remote_copy(
                src_ref=gbuf.at[r, at], dst_ref=gbuf.at[r, at], send_sem=gain_send.at[3 * r + k - 1], recv_sem=gain_recv.at[3 * r + k - 1],
                device_id=peer(axis, k), device_id_type=MESH,
            )
            for k in (1, 2, 3)
        ]

    def gain_received(r):
        axis = ("x", "y", "z")[r]
        at = (own["x"], own["y"], ring_z)[r]
        return [
            pltpu.make_async_remote_copy(
                src_ref=gbuf.at[r, at], dst_ref=gbuf.at[r, (at - k) % 4], send_sem=gain_send.at[3 * r + k - 1], recv_sem=gain_recv.at[3 * r + k - 1],
                device_id=peer(axis, k), device_id_type=MESH,
            )
            for k in (1, 2, 3)
        ]

    def gain_sum(r):
        for c in gain_received(r):
            c.wait()
        return (gbuf[r, 0] + gbuf[r, 1]) + (gbuf[r, 2] + gbuf[r, 3])

    def gain_tp():
        return pltpu.make_async_remote_copy(
            src_ref=gbuf.at[3, 0], dst_ref=gbuf.at[3, 1], send_sem=gain_send.at[9], recv_sem=gain_recv.at[9],
            device_id={"tp": 1 - tp}, device_id_type=MESH,
        )

    def gain_step(r):
        if r == 0:
            finish_input_gradient()
            for c in gain_copies(0):
                c.start()
        elif r < 3:
            gbuf[r, (own["x"], own["y"], ring_z)[r]] = gain_sum(r - 1)
            for c in gain_copies(r):
                c.start()
        elif r == 3:
            gbuf[3, 0] = gain_sum(2)
            gain_tp().start()
        else:
            gain_tp().wait()
            gain_tot[...] = gain_run[...] + factor * (gbuf[3, 0] + gbuf[3, 1])

    last = 4 + blocks - 1

    @pl.loop(0, last + 6)
    def _(t):
        def at_stage(offset, run_stage):
            j = t - offset

            @pl.when((j >= 0) & (j < blocks))
            def _():
                run_stage(j)

        for s in (5, 4, 3):
            at_stage(s - 1, functools.partial(ag_stage, s=s))
        at_stage(1, ag_second)

        for k in (0, 1):
            @pl.when(t == 1 + k)
            def _():
                ag_early(1, k)
        for k in range(5):
            @pl.when(t == k)
            def _():
                prepare(k)

        at_stage(4, backward)
        at_stage(10, choose(rs_finish, None))
        at_stage(9, choose(functools.partial(rs_stage, s=5), lambda j: rs_finish(j, lambda _: (once.at[4], once.at[5]))))
        at_stage(8, choose(functools.partial(rs_stage, s=4), rs_last_sum))
        at_stage(7, choose(functools.partial(rs_stage, s=3), rs_last_ring))
        at_stage(6, functools.partial(rs_stage, s=2))
        at_stage(5, functools.partial(rs_stage, s=1))
        at_stage(4, functools.partial(rs_stage, s=0))
        at_stage(4, later)
        at_stage(4, input_gradient)

        @pl.when(t == last)
        def _():
            send_input_gradient()

        for r in range(5):
            @pl.when(t == last + 1 + r)
            def _():
                gain_step(r)


def copy_kernel(*refs):
    n = len(refs) // 2
    copies = [pltpu.make_async_copy(a, b, refs[-1].at[i]) for i, (a, b) in enumerate(zip(refs[:n], refs[n : 2 * n]))]
    for c in copies:
        c.start()
    for c in copies:
        c.wait()


def copied(*arrays):
    n = len(arrays)
    return pl.pallas_call(
        copy_kernel,
        out_shape=tuple(jax.ShapeDtypeStruct(a.shape, a.dtype) for a in arrays),
        in_specs=[pl.BlockSpec(memory_space=pltpu.VMEM)] * n,
        out_specs=(pl.BlockSpec(memory_space=pl.ANY),) * n,
        scratch_shapes=[pltpu.SemaphoreType.DMA((n,))],
        compiler_params=pltpu.CompilerParams(vmem_limit_bytes=16 << 20),
        name="hand_over",
    )(*arrays)


def body(later_input, earlier_input, hidden_cot, norm_gain, gate_weight, up_weight, gate_running, up_running, gain_running):
    rows, width = later_input.shape
    shard, hidden = gate_weight.shape
    blocks = hidden // HALF
    quarter = shard // 4
    tokens = rows * lax.axis_size("rep") * lax.axis_size("fs") * lax.axis_size("tp")
    factor = 1.0 / math.sqrt(tokens)
    whole = (blocks, 2, 4, 4, shard, 2 * HALF)
    hbm = pl.BlockSpec(memory_space=pl.ANY)
    vmem = pl.BlockSpec(memory_space=pltpu.VMEM)
    dma = pltpu.SemaphoreType.DMA
    out = pl.pallas_call(
        functools.partial(kernel, blocks, factor),
        out_shape=(
            pltpu.VMEM((2 * rows, hidden), BF16),
            pltpu.VMEM((rows, width), BF16),
            pltpu.VMEM((shard, hidden), F32),
            pltpu.VMEM((shard, hidden), F32),
            pltpu.VMEM((1, width), F32),
        ),
        in_specs=[hbm, hbm, hbm, vmem, hbm, hbm, hbm, hbm, vmem],
        out_specs=(vmem, vmem, vmem, vmem, vmem),
        scratch_shapes=[
            pltpu.VMEM(whole, BF16),
            pltpu.VMEM(whole, BF16),
            pltpu.VMEM((2, rows, width), BF16),
            pltpu.VMEM((2, rows, width), BF16),
            pltpu.VMEM((2, rows, width), BF16),
            pltpu.VMEM((width, 2 * rows), BF16),
            pltpu.VMEM((2 * rows, hidden), BF16),
            pltpu.VMEM((2, rows, 2 * HALF), BF16),
            pltpu.VMEM((2, rows, width), F32),
            pltpu.VMEM((3, rows, width), BF16),
            pltpu.VMEM((rows, 1), F32),
            pltpu.VMEM((2, shard, hidden), F32),
            pltpu.VMEM((4, 4, 1, width), F32),
            pltpu.VMEM((blocks, shard, 2 * HALF), BF16),
            pltpu.VMEM((4, 3, quarter, 2 * HALF), BF16),
            *[pltpu.VMEM(s, BF16) for s in landing_shapes(ORDERS, blocks, quarter)],
            *[pltpu.VMEM(s, BF16) for s in landing_shapes(ORDERS_MID, 1, quarter)],
            dma((3, 3)),
            dma((3, 3, 3)),
            dma((2, 2, 2)),
            dma((3, 6)),
            dma((3, 3, 6)),
            dma((6,)),
            dma((5,)),
            dma((1,)),
            dma((4,)),
            dma((4,)),
            dma((2, 10)),
        ],
        compiler_params=pltpu.CompilerParams(collective_id=0, has_side_effects=True, vmem_limit_bytes=58 << 20),
        cost_estimate=pl.CostEstimate(flops=16 * rows * width * hidden * 2, bytes_accessed=16 << 20, transcendentals=0),
        name="half_step",
    )(
        later_input, earlier_input, hidden_cot, norm_gain.reshape(1, width), gate_weight, up_weight, gate_running, up_running,
        gain_running.reshape(1, width),
    )
    hidden_out, grad, gate_total, up_total, gain_total = copied(*out)
    return hidden_out, grad, gate_total, up_total, gain_total.reshape(width)


def solution(mesh):
    in_specs = (
        P(("rep", "fs", "tp"), None),
        P(("rep", "fs", "tp"), None),
        P(("rep", "fs"), "tp"),
        P(),
        P("fs", "tp"),
        P("fs", "tp"),
        P("fs", "tp"),
        P("fs", "tp"),
        P(),
    )
    out_specs = (
        P(("rep", "fs"), "tp"),
        P(("rep", "fs", "tp"), None),
        P("fs", "tp"),
        P("fs", "tp"),
        P(),
    )
    return jax.shard_map(body, mesh=mesh, in_specs=in_specs, out_specs=out_specs, check_vma=False)
```

```python
import functools
import math

import jax
import jax.numpy as jnp
from jax import lax
from jax.experimental import pallas as pl
from jax.experimental.pallas import tpu as pltpu
from jax.sharding import PartitionSpec as P

EPSILON = 1e-06
MESH = pl.DeviceIdType.MESH
HALF = 128
F32, BF16 = jnp.float32, jnp.bfloat16
SIZE = {"z": 2, "y": 4, "x": 4}
ORDERS = (("y", "z", "x"), ("x", "z", "y"), ("x", "y", "z"), ("y", "x", "z"))
ORDERS_MID = ORDERS[:2] + (("x", "z", "y"), ("y", "z", "x"))
ALL = slice(None)
AG_SHARDS = ((1, 1), (0.5, 0.5), (2, 4), (8, 2), (4, 8))
RS_SHARDS = ((4, 8), (8, 2), (2, 4), (0.5, 0.5), (1, 1))


def sigmoid(v):
    return 1.0 / (1.0 + jnp.exp(-v))


def landing_shapes(orders, blocks, quarter):
    shapes = []
    for order in orders:
        full = [a for a in "zyx"]
        for axis in reversed(order):
            full.remove(axis)
            lead = tuple(SIZE[a] for a in full)
            if axis == "z":
                shapes.append((blocks, 2, *lead, quarter, HALF))
            else:
                shapes.append((blocks, 2, *lead, quarter, HALF))
                shapes.append((blocks, 2, *lead, quarter, 2 * HALF))
    return shapes


def kernel(
    blocks, factor, later_hbm, earlier_hbm, cot_hbm, gain_ref, gw_hbm, uw_hbm, grun_hbm, urun_hbm, gain_run,
    hidden_out, grad_out, gtot_out, utot_out, gain_tot,
    w, g, xin, xl, xe, xt, cot, d, acc, dn, inv_ref, run, gbuf, rep_in, *rest,
):
    last_in, landing = rest[0], list(rest[1:-11])
    ag_send, ag_recv, early, rs_send, rs_recv, once, load_sem, w_sem, tp_send, tp_recv, gs = rest[-11:]
    gain_send, gain_recv = gs.at[0], gs.at[1]
    rows = xin.shape[1]
    width = xin.shape[2]
    quarter = g.shape[4] // 4
    rep, fs, tp = lax.axis_index("rep"), lax.axis_index("fs"), lax.axis_index("tp")
    own = {"x": fs % 4, "y": (fs // 4) % 4, "z": fs // 16}
    ring_z = 2 * rep + own["z"]

    def peer(axis, by):
        if axis == "z":
            z = (ring_z + by) % 4
            return {"rep": z // 2, "fs": (z % 2) * 16 + own["y"] * 4 + own["x"]}
        c = (own[axis] + by) % 4
        if axis == "y":
            return {"fs": own["z"] * 16 + c * 4 + own["x"]}
        return {"fs": own["z"] * 16 + own["y"] * 4 + c}

    def shifted(axis, by):
        return (1 - own["z"] if by else own["z"]) if axis == "z" else (own[axis] + by) % 4

    HALVES = (pl.ds(0, HALF), pl.ds(HALF, HALF), pl.ds(0, 2 * HALF))

    def region(j, q, sel, half):
        return (j, sel["z"], sel["y"], sel["x"], pl.ds(q * quarter, quarter), HALVES[half])

    def sel_of(full, axis, coordinate):
        s = {a: (ALL if a in full else own[a]) for a in "zyx"}
        s[axis] = coordinate
        return s

    def plan_gather(orders):
        plans, count = [], 0
        for q, order in enumerate(orders):
            phases = []
            for p, axis in enumerate(order):
                full = order[:p]
                if axis == "z":
                    group = []
                    for k, by in enumerate((1, -1)):
                        group.append((count, (q, sel_of(full, "z", own["z"]), k), ("z", by), (q, sel_of(full, "z", 1 - own["z"]), k)))
                        count += 1
                    phases.append(("z", [group]))
                else:
                    first, second = [], []
                    for k, by in enumerate((1, -1)):
                        first.append((count, (q, sel_of(full, axis, own[axis]), 2), (axis, by), (q, sel_of(full, axis, shifted(axis, -by)), 2)))
                        count += 1
                    for k, by in enumerate((1, -1)):
                        second.append((count, (q, sel_of(full, axis, shifted(axis, -by)), k), (axis, by), (q, sel_of(full, axis, shifted(axis, 2)), k)))
                        count += 1
                    phases.append((axis, [first, second]))
            plans.append([group for _, groups in phases for group in groups])
        return plans

    ag_plans = plan_gather(ORDERS), plan_gather(ORDERS_MID)
    ag_plan = ag_plans[0]

    def shards(n):
        if n <= 4:
            if n == 0.5:
                return w.at[0, 0, 0, 0, pl.ds(0, 2 * quarter)]
            return w.at[0, 0, 0, pl.ds(0, n)]
        if n % 4 == 0:
            return w.at[0, 0, pl.ds(0, n // 4)]
        return w.at[:, 0, 0, 0]

    def await_stage(n, send, recv):
        pltpu.make_async_copy(shards(n), shards(n), send).wait()
        pltpu.make_async_copy(shards(n), shards(n), recv).wait()

    def ag_send_to(j, src, to, send, recv):
        pltpu.make_async_remote_copy(
            src_ref=w.at[region(j, *src)], dst_ref=w.at[region(j, *src)], send_sem=send, recv_sem=recv, device_id=peer(*to), device_id_type=MESH
        ).start()

    middle = blocks // 2

    def per_kind(j, pair, run):
        if pair == 0:
            run(0)
            return

        @pl.when(j != middle)
        def _():
            run(0)

        @pl.when(j == middle)
        def _():
            run(1)

    def ag_stage(j, s, wait=True):
        for pair in (1, 0):
            def part(kind):
                if wait:
                    await_stage(AG_SHARDS[s - 1][0 if kind else pair], ag_send.at[pair + kind, s - 3], ag_recv.at[j % 3, pair + kind, s - 3])
                if s < 5:
                    for plan in ag_plans[kind][2 * pair : 2 * pair + 2]:
                        for _, src, to, _ in plan[s]:
                            ag_send_to(j, src, to, ag_send.at[pair + kind, s - 2], ag_recv.at[j % 3, pair + kind, s - 2])

            per_kind(j, pair, part)

    def ag_first():
        for q, order in enumerate(ORDERS):
            src = (q, sel_of((), order[0], own[order[0]]), 2)
            for by in (2, 1, -1):
                ag_send_to(0, src, (order[0], by), once.at[0], once.at[1])

    groups = (pl.ds(1, 1), pl.ds(2, blocks - 2))

    def ag_early(s, k):
        if s == 1:
            await_early(0, k)
        for plan in ag_plan:
            for _, src, to, _ in plan[s]:
                ag_send_to(groups[k], src, to, early.at[k, 0, s], early.at[k, 1, s])

    def await_early(s, k):
        for way in (0, 1):
            view = w.at[groups[k], 0, 0, pl.ds(0, 2)] if s == 0 else w.at[groups[k], 0, 0, 0]
            pltpu.make_async_copy(view, view, early.at[k, way, s]).wait()

    def ag_second(j):
        @pl.when(j == 0)
        def _():
            await_stage(3, once.at[0], once.at[1])

        for k in (0, 1):
            @pl.when(j == 1 + k)
            def _():
                await_early(1, k)

        ag_stage(j, 2, wait=False)

    def plan_scatter(orders, place):
        plans, count = [], 0
        for q, order in enumerate(orders):
            groups = []
            full = ["z", "y", "x"]
            for axis in reversed(order):
                full.remove(axis)
                if axis == "z":
                    group = []
                    for k, by in enumerate((1, -1)):
                        group.append((count, (q, sel_of(full, "z", 1 - own["z"]), k), ("z", by), place, k, (q, sel_of(full, "z", own["z"]), k)))
                        count += 1
                    groups.append(group)
                    place += 1
                else:
                    first, second = [], []
                    for k, by in enumerate((1, -1)):
                        first.append((count, (q, sel_of(full, axis, shifted(axis, 2)), k), (axis, by), place, k, (q, sel_of(full, axis, shifted(axis, by)), k)))
                        count += 1
                    for k, by in enumerate((1, -1)):
                        second.append((count, (q, sel_of(full, axis, shifted(axis, by)), 2), (axis, by), place + 1, k, (q, sel_of(full, axis, own[axis]), 2)))
                        count += 1
                    groups += [first, second]
                    place += 2
            plans.append(groups)
        return plans

    half_landing = len(landing) // 2
    rs_plans = plan_scatter(ORDERS, 0), plan_scatter(ORDERS_MID, half_landing)

    def land(kind, j, at, slot):
        return landing[at].at[0 if kind else j, slot]

    def rs_start(j, s, pair, kind, t):
        _, src, to, at, slot, _ = t
        pltpu.make_async_remote_copy(
            src_ref=g.at[region(j, *src)], dst_ref=land(kind, j, at, slot), send_sem=rs_send.at[pair + kind, s],
            recv_sem=rs_recv.at[j % 3, pair + kind, s], device_id=peer(*to), device_id_type=MESH,
        ).start()

    def rep_copy(j, send, recv):
        return pltpu.make_async_remote_copy(
            src_ref=g.at[j, own["z"], own["y"], own["x"]], dst_ref=rep_in.at[j], send_sem=send, recv_sem=recv,
            device_id=peer("z", 2), device_id_type=MESH,
        )

    def rep_sems(j):
        return rs_send.at[0, 5], rs_recv.at[j % 3, 0, 5]

    def rs_collect(j, s, pair, kind=0):
        await_stage(RS_SHARDS[s - 1][0 if kind else pair], rs_send.at[pair + kind, s - 1], rs_recv.at[j % 3, pair + kind, s - 1])
        for plan in rs_plans[kind][2 * pair : 2 * pair + 2]:
            for _, _, _, at, slot, target in plan[s - 1]:
                to = region(j, *target)
                g[to] = (g[to].astype(F32) + land(kind, j, at, slot)[...].astype(F32)).astype(BF16)

    def rs_stage(j, s):
        for pair in (1, 0) if s in (2, 4) else (0, 1):
            def part(kind):
                if s >= 1:
                    rs_collect(j, s, pair, kind)
                if s < 5:
                    for plan in rs_plans[kind][2 * pair : 2 * pair + 2]:
                        for t in plan[s]:
                            rs_start(j, s, pair, kind, t)

            per_kind(j, pair, part)
        if s == 5:
            rep_copy(j, *rep_sems(j)).start()

    def rs_last_ring(j):
        for pair in (0, 1):
            rs_collect(j, 3, pair)
            for q in (2 * pair, 2 * pair + 1):
                axis = ORDERS[q][0]
                for k, by in enumerate((2, 1, -1)):
                    pltpu.make_async_remote_copy(
                        src_ref=g.at[region(j, q, sel_of((), axis, shifted(axis, by)), 2)], dst_ref=last_in.at[q, k],
                        send_sem=once.at[2], recv_sem=once.at[3], device_id=peer(axis, by), device_id_type=MESH,
                    ).start()

    def rs_last_sum(j):
        await_stage(3, once.at[2], once.at[3])
        for q, order in enumerate(ORDERS):
            to = region(j, q, sel_of((), order[0], own[order[0]]), 2)
            g[to] = (g[to].astype(F32) + last_in[q, 0].astype(F32) + last_in[q, 1].astype(F32) + last_in[q, 2].astype(F32)).astype(BF16)
        rep_copy(j, once.at[4], once.at[5]).start()

    def choose(usual, for_last):
        def stage(j):
            if usual is not None:
                @pl.when(j < blocks - 1)
                def _():
                    usual(j)

            if for_last is not None:
                @pl.when(j == blocks - 1)
                def _():
                    for_last(j)

        return stage

    def rs_finish(j, sems=rep_sems):
        rep_copy(j, *sems(j)).wait()
        total = g[j, own["z"], own["y"], own["x"]].astype(F32) + rep_in[j].astype(F32)
        columns = pl.ds(pl.multiple_of(j * HALF, HALF), HALF)
        gtot_out[:, columns] = run[0, :, columns] + factor * total[:, :HALF]
        utot_out[:, columns] = run[1, :, columns] + factor * total[:, HALF:]

    def tp_copy(i, ref):
        return pltpu.make_async_remote_copy(
            src_ref=ref, dst_ref=ref, send_sem=tp_send.at[i], recv_sem=tp_recv.at[i], device_id={"tp": 1 - tp}, device_id_type=MESH
        )

    def tp_received(i, ref):
        return pltpu.make_async_remote_copy(
            src_ref=ref, dst_ref=ref, send_sem=tp_send.at[i], recv_sem=tp_recv.at[i], device_id={"tp": 1 - tp}, device_id_type=MESH
        )

    def dn_copy():
        return pltpu.make_async_remote_copy(
            src_ref=dn.at[1], dst_ref=dn.at[2], send_sem=tp_send.at[3], recv_sem=tp_recv.at[3], device_id={"tp": 1 - tp}, device_id_type=MESH
        )

    loads = [
        pltpu.make_async_copy(later_hbm, xin.at[0], load_sem.at[0]),
        pltpu.make_async_copy(earlier_hbm, xin.at[1], load_sem.at[1]),
        pltpu.make_async_copy(cot_hbm, cot, load_sem.at[2]),
        pltpu.make_async_copy(grun_hbm, run.at[0], load_sem.at[3]),
        pltpu.make_async_copy(urun_hbm, run.at[1], load_sem.at[4]),
    ]

    def shard_loads(j):
        columns = pl.ds(pl.multiple_of(j * HALF, HALF), HALF)
        mine = (j, own["z"], own["y"], own["x"], ALL)
        return [
            pltpu.make_async_copy(gw_hbm.at[:, columns], w.at[(*mine, pl.ds(0, HALF))], w_sem.at[0]),
            pltpu.make_async_copy(uw_hbm.at[:, columns], w.at[(*mine, pl.ds(HALF, HALF))], w_sem.at[0]),
        ]

    @pl.loop(0, blocks)
    def _(j):
        for c in shard_loads(j):
            c.start()

    for c in loads:
        c.start()

    barrier = pltpu.get_barrier_semaphore()
    greeted = [peer(a, by) for a in "xyz" for by in (1, 2, 3)] + [{"tp": 1 - tp}]
    for device in greeted:
        pl.semaphore_signal(barrier, inc=1, device_id=device, device_id_type=MESH)
    pl.semaphore_wait(barrier, len(greeted))

    pltpu.make_async_copy(w.at[:, own["z"], own["y"], own["x"]], w.at[:, own["z"], own["y"], own["x"]], w_sem.at[0]).wait()
    ag_first()
    ag_early(0, 0)
    ag_early(0, 1)

    step_rows = 32 if rows % 32 == 0 else rows

    def normalize(m, out):
        @pl.loop(0, rows // step_rows)
        def _(i):
            at = pl.ds(pl.multiple_of(i * step_rows, step_rows), step_rows)
            values = xin[m, at, :].astype(F32)
            inv = lax.rsqrt(jnp.mean(values * values, axis=1, keepdims=True) + EPSILON)
            out[tp, at, :] = (values * inv * gain_ref[...]).astype(BF16)
            if m == 1:
                inv_ref[at, :] = inv

    def prepare(t):
        if t == 0:
            for c in loads:
                c.wait()
            normalize(1, xe)
            tp_copy(1, xe.at[tp]).start()
        elif t == 1:
            slab, mine = min(256, width), pl.ds(pl.multiple_of(tp * rows, rows), rows)

            @pl.loop(0, width // slab)
            def _(i):
                at = pl.ds(pl.multiple_of(i * slab, slab), slab)
                xt[at, mine] = xe[tp, :, at].T

            tp_copy(2, xt.at[:, mine]).start()
        elif t == 2:
            normalize(0, xl)
            tp_copy(0, xl.at[tp]).start()
        elif t == 3:
            acc[...] = jnp.zeros_like(acc)
        else:
            exchanged()

    def exchanged():
        for i, ref in ((0, xl), (1, xe)):
            tp_copy(i, ref.at[tp]).wait_send()
            tp_received(i, ref.at[1 - tp]).wait_recv()
        tp_copy(2, xt.at[:, pl.ds(pl.multiple_of(tp * rows, rows), rows)]).wait_send()
        tp_received(2, xt.at[:, pl.ds(pl.multiple_of((1 - tp) * rows, rows), rows)]).wait_recv()

    def block_weight(j):
        return w[j].reshape(width, 2 * HALF)

    def backward(j):
        columns = pl.ds(pl.multiple_of(j * HALF, HALF), HALF)

        for m in range(2):
            both = jnp.dot(xe[m], block_weight(j), preferred_element_type=F32)
            gate, up = both[:, :HALF], both[:, HALF:]
            s = sigmoid(gate)
            c = cot[pl.ds(m * rows, rows), columns].astype(F32)
            d[m, :, 0:HALF] = (c * up * s * (1.0 + gate * (1.0 - s))).astype(BF16)
            d[m, :, HALF:] = (c * gate * s).astype(BF16)

        for k in range(4):
            z, y = k // 2, 2 * (k % 2)
            at = pl.ds(k * (width // 4), width // 4)
            part = jnp.dot(xt[at, :], d[...].reshape(2 * rows, 2 * HALF), preferred_element_type=F32)
            g[j, z, pl.ds(y, 2)] = part.astype(BF16).reshape(2, 4, 4 * quarter, 2 * HALF)

    def later(j):
        columns = pl.ds(pl.multiple_of(j * HALF, HALF), HALF)

        @pl.loop(0, 2)
        def _(m):
            both = jnp.dot(xl[m], block_weight(j), preferred_element_type=F32)
            gate, up = both[:, :HALF], both[:, HALF:]
            hidden_out[pl.ds(pl.multiple_of(m * rows, rows), rows), columns] = (gate * sigmoid(gate) * up).astype(BF16)

    def input_gradient(j):
        @pl.loop(0, 4)
        def _(k):
            z, y = k // 2, 2 * (k % 2)
            at = pl.ds(pl.multiple_of(k * (width // 4), width // 4), width // 4)
            part = w[j, z, pl.ds(y, 2)].reshape(width // 4, 2 * HALF)
            for m in range(2):
                acc[m, :, at] = acc[m, :, at] + lax.dot_general(
                    d[m], part, (((1,), (1,)), ((), ())), preferred_element_type=F32
                )

    def send_input_gradient():
        @pl.loop(0, rows // step_rows)
        def _(i):
            at = pl.ds(pl.multiple_of(i * step_rows, step_rows), step_rows)
            dn[0, at, :] = acc[tp, at, :].astype(BF16)
            dn[1, at, :] = acc[1 - tp, at, :].astype(BF16)

        dn_copy().start()

    def finish_input_gradient():
        dn_copy().wait()
        gain = gain_ref[...]
        own_slot = gbuf.at[0, own["x"]]
        own_slot[...] = jnp.zeros_like(own_slot)

        @pl.loop(0, rows // step_rows)
        def _(i):
            at = pl.ds(pl.multiple_of(i * step_rows, step_rows), step_rows)
            d_norm = dn[0, at, :].astype(F32) + dn[2, at, :].astype(F32)
            values = xin[1, at, :].astype(F32)
            inv = inv_ref[at, :]
            scaled = d_norm * gain
            inner = jnp.mean(scaled * values, axis=1, keepdims=True)
            grad_out[at, :] = (inv * scaled - values * (inv * inv * inv) * inner).astype(BF16)
            own_slot[...] = own_slot[...] + jnp.sum(d_norm * values * inv, axis=0, keepdims=True)

    def gain_copies(r):
        axis = ("x", "y", "z")[r]
        at = (own["x"], own["y"], ring_z)[r]
        return [
            pltpu.make_async_remote_copy(
                src_ref=gbuf.at[r, at], dst_ref=gbuf.at[r, at], send_sem=gain_send.at[3 * r + k - 1], recv_sem=gain_recv.at[3 * r + k - 1],
                device_id=peer(axis, k), device_id_type=MESH,
            )
            for k in (1, 2, 3)
        ]

    def gain_received(r):
        axis = ("x", "y", "z")[r]
        at = (own["x"], own["y"], ring_z)[r]
        return [
            pltpu.make_async_remote_copy(
                src_ref=gbuf.at[r, at], dst_ref=gbuf.at[r, (at - k) % 4], send_sem=gain_send.at[3 * r + k - 1], recv_sem=gain_recv.at[3 * r + k - 1],
                device_id=peer(axis, k), device_id_type=MESH,
            )
            for k in (1, 2, 3)
        ]

    def gain_sum(r):
        for c in gain_received(r):
            c.wait()
        return (gbuf[r, 0] + gbuf[r, 1]) + (gbuf[r, 2] + gbuf[r, 3])

    def gain_tp():
        return pltpu.make_async_remote_copy(
            src_ref=gbuf.at[3, 0], dst_ref=gbuf.at[3, 1], send_sem=gain_send.at[9], recv_sem=gain_recv.at[9],
            device_id={"tp": 1 - tp}, device_id_type=MESH,
        )

    def gain_step(r):
        if r == 0:
            finish_input_gradient()
            for c in gain_copies(0):
                c.start()
        elif r < 3:
            gbuf[r, (own["x"], own["y"], ring_z)[r]] = gain_sum(r - 1)
            for c in gain_copies(r):
                c.start()
        elif r == 3:
            gbuf[3, 0] = gain_sum(2)
            gain_tp().start()
        else:
            gain_tp().wait()
            gain_tot[...] = gain_run[...] + factor * (gbuf[3, 0] + gbuf[3, 1])

    last = 4 + blocks - 1

    @pl.loop(0, last + 6)
    def _(t):
        def at_stage(offset, run_stage):
            j = t - offset

            @pl.when((j >= 0) & (j < blocks))
            def _():
                run_stage(j)

        for s in (5, 4, 3):
            at_stage(s - 1, functools.partial(ag_stage, s=s))
        at_stage(1, ag_second)

        @pl.when(t == 1)
        def _():
            ag_early(1, 0)
        for k in range(5):
            @pl.when(t == k)
            def _():
                prepare(k)
                if k == 1:
                    ag_early(1, 1)

        at_stage(4, backward)
        at_stage(10, choose(rs_finish, None))
        at_stage(9, choose(functools.partial(rs_stage, s=5), lambda j: rs_finish(j, lambda _: (once.at[4], once.at[5]))))
        at_stage(8, choose(functools.partial(rs_stage, s=4), rs_last_sum))
        at_stage(7, choose(functools.partial(rs_stage, s=3), rs_last_ring))
        at_stage(6, functools.partial(rs_stage, s=2))
        at_stage(5, functools.partial(rs_stage, s=1))
        at_stage(4, functools.partial(rs_stage, s=0))
        at_stage(4, later)
        at_stage(4, input_gradient)

        @pl.when(t == last)
        def _():
            send_input_gradient()

        for r in range(5):
            @pl.when(t == last + 1 + r)
            def _():
                gain_step(r)


def copy_kernel(*refs):
    n = len(refs) // 2
    copies = [pltpu.make_async_copy(a, b, refs[-1].at[i]) for i, (a, b) in enumerate(zip(refs[:n], refs[n : 2 * n]))]
    for c in copies:
        c.start()
    for c in copies:
        c.wait()


def copied(*arrays):
    n = len(arrays)
    return pl.pallas_call(
        copy_kernel,
        out_shape=tuple(jax.ShapeDtypeStruct(a.shape, a.dtype) for a in arrays),
        in_specs=[pl.BlockSpec(memory_space=pltpu.VMEM)] * n,
        out_specs=(pl.BlockSpec(memory_space=pl.ANY),) * n,
        scratch_shapes=[pltpu.SemaphoreType.DMA((n,))],
        compiler_params=pltpu.CompilerParams(vmem_limit_bytes=16 << 20),
        name="hand_over",
    )(*arrays)


def body(later_input, earlier_input, hidden_cot, norm_gain, gate_weight, up_weight, gate_running, up_running, gain_running):
    rows, width = later_input.shape
    shard, hidden = gate_weight.shape
    blocks = hidden // HALF
    quarter = shard // 4
    tokens = rows * lax.axis_size("rep") * lax.axis_size("fs") * lax.axis_size("tp")
    factor = 1.0 / math.sqrt(tokens)
    whole = (blocks, 2, 4, 4, shard, 2 * HALF)
    hbm = pl.BlockSpec(memory_space=pl.ANY)
    vmem = pl.BlockSpec(memory_space=pltpu.VMEM)
    dma = pltpu.SemaphoreType.DMA
    out = pl.pallas_call(
        functools.partial(kernel, blocks, factor),
        out_shape=(
            pltpu.VMEM((2 * rows, hidden), BF16),
            pltpu.VMEM((rows, width), BF16),
            pltpu.VMEM((shard, hidden), F32),
            pltpu.VMEM((shard, hidden), F32),
            pltpu.VMEM((1, width), F32),
        ),
        in_specs=[hbm, hbm, hbm, vmem, hbm, hbm, hbm, hbm, vmem],
        out_specs=(vmem, vmem, vmem, vmem, vmem),
        scratch_shapes=[
            pltpu.VMEM(whole, BF16),
            pltpu.VMEM(whole, BF16),
            pltpu.VMEM((2, rows, width), BF16),
            pltpu.VMEM((2, rows, width), BF16),
            pltpu.VMEM((2, rows, width), BF16),
            pltpu.VMEM((width, 2 * rows), BF16),
            pltpu.VMEM((2 * rows, hidden), BF16),
            pltpu.VMEM((2, rows, 2 * HALF), BF16),
            pltpu.VMEM((2, rows, width), F32),
            pltpu.VMEM((3, rows, width), BF16),
            pltpu.VMEM((rows, 1), F32),
            pltpu.VMEM((2, shard, hidden), F32),
            pltpu.VMEM((4, 4, 1, width), F32),
            pltpu.VMEM((blocks, shard, 2 * HALF), BF16),
            pltpu.VMEM((4, 3, quarter, 2 * HALF), BF16),
            *[pltpu.VMEM(s, BF16) for s in landing_shapes(ORDERS, blocks, quarter)],
            *[pltpu.VMEM(s, BF16) for s in landing_shapes(ORDERS_MID, 1, quarter)],
            dma((3, 3)),
            dma((3, 3, 3)),
            dma((2, 2, 2)),
            dma((3, 6)),
            dma((3, 3, 6)),
            dma((6,)),
            dma((5,)),
            dma((1,)),
            dma((4,)),
            dma((4,)),
            dma((2, 10)),
        ],
        compiler_params=pltpu.CompilerParams(collective_id=0, has_side_effects=True, vmem_limit_bytes=58 << 20),
        cost_estimate=pl.CostEstimate(flops=16 * rows * width * hidden * 2, bytes_accessed=16 << 20, transcendentals=0),
        name="half_step",
    )(
        later_input, earlier_input, hidden_cot, norm_gain.reshape(1, width), gate_weight, up_weight, gate_running, up_running,
        gain_running.reshape(1, width),
    )
    hidden_out, grad, gate_total, up_total, gain_total = copied(*out)
    return hidden_out, grad, gate_total, up_total, gain_total.reshape(width)


def solution(mesh):
    in_specs = (
        P(("rep", "fs", "tp"), None),
        P(("rep", "fs", "tp"), None),
        P(("rep", "fs"), "tp"),
        P(),
        P("fs", "tp"),
        P("fs", "tp"),
        P("fs", "tp"),
        P("fs", "tp"),
        P(),
    )
    out_specs = (
        P(("rep", "fs"), "tp"),
        P(("rep", "fs", "tp"), None),
        P("fs", "tp"),
        P("fs", "tp"),
        P(),
    )
    return jax.shard_map(body, mesh=mesh, in_specs=in_specs, out_specs=out_specs, check_vma=False)
```
